32 devices in a mesh: grp: 2 (over y), ep: 8 (over z, x), tp: 2 (over core).
Axes of the slice: x: 2, y: 2, z: 4, core: 2. Of those that a mesh axis runs over, the one named last changes fastest.
Arguments:
- tokens: bfloat16 [2048, 2048], P(('grp', 'ep')), parts along dimension 0, may hold values from -6 to 6
- in_gain: float32 [2048], replicated, may hold values from 0.1 to 1.9
- routing: int32 [2048, 4], P(('grp', 'ep')), parts along dimension 0, may hold values from 0 to 15, as said below
- gate_prob: float32 [2048, 4], P(('grp', 'ep')), parts along dimension 0, may hold values from 0.05 to 1
- w_gate: bfloat16 [16, 2048, 512], P('ep', None, 'tp'), may hold values from -0.125 to 0.125
- w_up: bfloat16 [16, 2048, 512], P('ep', None, 'tp'), may hold values from -0.125 to 0.125
- w_down: bfloat16 [16, 512, 2048], P('ep', 'tp')
- out_gain: float32 [2048], P('tp'), may hold values from 0.1 to 1.9
Outputs:
- output: bfloat16 [2048, 2048], P(('grp', 'ep'), 'tp'), parts along dimension 0
The draws below stay inside these ranges and needn't reach their ends.
There are 2 independent parts, one for each index of `grp`. The reference program is written for one: setup_inputs(seed, part) draws one part's arguments, and reference() takes and returns one part's arrays. A program takes and returns all parts, laid end to end along the dimension named above; an argument that names none is the same for every part. Nothing has to cross between parts.
Inputs may be any that keep to these rules, and one draw needn't show every extreme that they name: `routing`: each row names 4 different experts, all of one group (the same value of expert // 4). In the rows of one device no expert is named more than 64 times, and in every device's rows some expert is named exactly 64 times.
All inputs are finite; a program needn't handle non-finite values.
Results may differ from the reference program's by a relative error of at most 0.0077.
Values may be sent and summed in bfloat16 or wider, within the bound.
A program may use at most 64 MiB of HBM per device.

```python
import math
import jax
import jax.numpy as jnp
from jax import lax

D = 2048
FF = 512
GROUPS = 4
TOPK = 4
TOK_DEV = 128
EXPERTS = 16
EPG = 4
TOKENS = 1024
CAP = 64
GMAX = 64
N_EP = 8
N_TP = 2


def draw_routing(key, part):
    block_count = TOKENS // TOK_DEV
    key_order, key_pick, key_perm, key_shuffle = jax.random.split(key, 4)
    hot_count = min(GMAX, TOK_DEV)
    hot_span = hot_count * TOPK // CAP
    group_order = jax.random.permutation(key_order, GROUPS)
    hot_picks = jnp.minimum(jax.random.randint(key_pick, (block_count,), 0, GROUPS + 2), GROUPS - 1)
    hot_group = group_order[hot_picks]
    position = jnp.arange(TOK_DEV, dtype=jnp.int32)
    is_hot = position < hot_count
    cold_index = position - hot_count
    groups = jnp.where(is_hot[None, :], hot_group[:, None], (hot_group[:, None] + 1 + cold_index[None, :] % (GROUPS - 1)) % GROUPS)
    group_rank = jnp.where(is_hot, position, cold_index // (GROUPS - 1))
    modulus = jnp.where(is_hot, hot_span, EPG)
    within = (group_rank[:, None] * TOPK + jnp.arange(TOPK, dtype=jnp.int32)[None, :]) % modulus[:, None]
    perm_keys = jax.random.split(key_perm, block_count * GROUPS)
    orders = jax.vmap(lambda one_key: jax.random.permutation(one_key, EPG))(perm_keys).reshape(block_count, GROUPS, EPG)
    block_ids = jnp.arange(block_count)[:, None, None]
    local_ids = orders[block_ids, groups[:, :, None], within[None, :, :]]
    experts = groups[:, :, None] * EPG + local_ids
    shuffle_keys = jax.random.split(key_shuffle, block_count)
    shuffles = jax.vmap(lambda one_key: jax.random.permutation(one_key, TOK_DEV))(shuffle_keys)
    experts = jnp.take_along_axis(experts, shuffles[:, :, None], axis=1)
    return experts.reshape(TOKENS, TOPK).astype(jnp.int32)


def draw_w_down(key, part):
    key_base, key_col = jax.random.split(key)
    columns = jnp.arange(D, dtype=jnp.float32) / D
    entries_base = jax.random.normal(key_base, (EXPERTS, FF, D), jnp.float32)
    spread = jax.random.uniform(key_col, (D,), jnp.float32, 0.5, 1.5)
    col_rise = 3.0 ** columns
    return (entries_base * FF ** (-0.5) * col_rise * spread).astype(jnp.bfloat16)


def levels(own_key, dims, cuts, low, largest):
    def one(dim, parts):
        draws = jax.random.uniform(jax.random.fold_in(jax.random.fold_in(own_key, 6), dim), (parts,), jnp.float32, low / len(cuts), largest / len(cuts))
        return jnp.repeat(jnp.exp(draws), dims[dim] // parts).reshape((-1,) + (1,) * (len(dims) - dim - 1))

    gain = one(*cuts[0])
    for cut in cuts[1:]:
        gain = gain * one(*cut)
    return gain


def bell_draw(rng, extent, width, most, cuts=(), kind=jnp.bfloat16):
    result = jax.random.normal(rng, extent, jnp.float32) * width
    if len(cuts) > 0:
        result = levels(rng, extent, cuts, -0.22, 0.18) * result
    return jnp.clip(result, min=-most, max=most).astype(kind)


def setup_inputs(seed: int = 0, part: int = 0) -> dict:
    seeds = jax.random.split(jax.random.key(seed), 9)
    part_keys = jax.random.split(jax.random.fold_in(seeds[8], part), 9)
    tokens = bell_draw(part_keys[0], (TOKENS, D), 1.0, 6.0, ((0, 8),))
    in_gain = jnp.clip(1.0 + 0.18 * jax.random.normal(seeds[1], (D,), jnp.float32), 0.1, 1.9)
    routing = draw_routing(jax.random.fold_in(jax.random.fold_in(seeds[8], part), 71), part)
    gate_prob = jnp.clip(jnp.exp(math.log(1.0) - 2.9957323 * jax.random.uniform(part_keys[3], (TOKENS, TOPK), jnp.float32) ** levels(part_keys[3], (TOKENS, TOPK), ((0, 8),), -0.2, 0.2)), 0.05, 1.0)
    w_gate = bell_draw(seeds[4], (EXPERTS, D, FF), D ** -0.5, 0.125, ((0, 8), (2, 2)))
    w_up = bell_draw(seeds[5], (EXPERTS, D, FF), D ** -0.5, 0.125, ((0, 8), (2, 2)))
    w_down = draw_w_down(jax.random.fold_in(seeds[8], 71), part)
    out_gain = jnp.clip(1.0 + 0.18 * jax.random.normal(seeds[7], (D,), jnp.float32), 0.1, 1.9)
    return dict(tokens=tokens, in_gain=in_gain, routing=routing, gate_prob=gate_prob, w_gate=w_gate, w_up=w_up, w_down=w_down, out_gain=out_gain)


EPS = 1e-06

def slot_ranks(flat_routes):
    matches = (flat_routes[:, None] == jnp.arange(EXPERTS, dtype=jnp.int32)[None, :]).astype(jnp.int32)
    earlier = jnp.cumsum(matches, axis=0) - matches
    return lax.optimization_barrier(jnp.sum(earlier * matches, axis=1)).astype(jnp.int32)

def reference(tokens, in_gain, routing, gate_prob, w_gate, w_up, w_down, out_gain):
    floats = tokens.astype(jnp.float32)
    normed = (floats * lax.rsqrt(lax.optimization_barrier(jnp.mean(floats * floats, axis=-1, keepdims=True)) + EPS) * in_gain).astype(jnp.bfloat16)
    blocks = routing.reshape(N_EP, TOK_DEV * TOPK)
    slot_rank = jax.vmap(slot_ranks)(blocks)
    sources = jnp.arange(N_EP, dtype=jnp.int32)[:, None]
    slot_ids = (blocks * (N_EP * CAP) + sources * CAP + slot_rank).reshape(-1).astype(jnp.int32)
    token_ids = jnp.arange(TOKENS * TOPK, dtype=jnp.int32) // TOPK
    slot_table = jnp.zeros((EXPERTS * N_EP * CAP,), jnp.int32).at[slot_ids].set(token_ids + 1)
    slot_table = slot_table.reshape(EXPERTS, N_EP * CAP)

    def expert(inputs):
        entries, gate_w, up_w, down_w = inputs
        filled = entries > 0
        rows_in = jnp.where(filled[:, None], normed[jnp.maximum(entries - 1, 0)], jnp.zeros((), jnp.bfloat16))
        gate_act = jnp.dot(rows_in, gate_w, preferred_element_type=jnp.float32)
        up_act = jnp.dot(rows_in, up_w, preferred_element_type=jnp.float32)
        hidden = (jax.nn.silu(gate_act) * up_act).astype(jnp.bfloat16)
        pieces = jnp.einsum('rnf,nfd->nrd', hidden.reshape(-1, N_TP, FF // N_TP).astype(jnp.float32), down_w.reshape(N_TP, FF // N_TP, D).astype(jnp.float32))
        rounded = lax.optimization_barrier(pieces.astype(jnp.bfloat16))
        return lax.optimization_barrier(jnp.sum(rounded.astype(jnp.float32), axis=0)).astype(jnp.bfloat16)
    results = lax.map(expert, (slot_table, w_gate, w_up, w_down))
    picked = results.reshape(-1, D)[slot_ids].astype(jnp.float32).reshape(TOKENS, TOPK, D)
    mixed_rows = lax.optimization_barrier(jnp.sum(picked * gate_prob[:, :, None], axis=1))
    inv_rms = lax.rsqrt(lax.optimization_barrier(jnp.mean(mixed_rows * mixed_rows, axis=-1, keepdims=True)) + EPS)
    return (mixed_rows * inv_rms * out_gain).astype(jnp.bfloat16)
```

```python
import functools

import jax
import jax.numpy as jnp
from jax import lax
from jax.experimental import pallas as pl
from jax.experimental.pallas import tpu as pltpu
from jax.sharding import PartitionSpec as P

GROUPS = 4
EPS = 1e-06
MESH = pl.DeviceIdType.MESH
F32 = jnp.float32
BF16 = jnp.bfloat16

STEPS = (
    "A11", "B01", "A10", "B00", "G01", "B11", "G00", "A21", "B10", "G11", "A20", "G10",
    "D11", "D10", "B21", "A31", "G21", "D01", "B20", "G20", "D00", "A30", "F11", "F10",
    "D21", "B31", "D20", "G31", "B30", "D31", "G30", "F21", "D30", "F20", "F01", "F00",
    "M01", "M00", "F31", "F30", "M11", "M10", "M21", "M20", "M31", "M30",
)


def loop(low, high, step):
    if high - low <= 8:
        for i in range(low, high):
            step(i)
    else:
        lax.fori_loop(low, high, lambda i, carry: (step(i), carry)[1], 0)


def partner(q, d, count):
    if count & (count - 1):
        return lax.rem(q + d, count), lax.rem(q + count - d, count)
    other, bit = 0, 1
    while bit < count:
        mine, theirs = (q // bit) % 2, (d // bit) % 2
        other = other + bit * (mine + theirs - 2 * mine * theirs)
        bit *= 2
    return other, other


def kernel(
    group_count, span, rows,
    routes_ref, probs_ref, in_gain_ref, out_gain_ref, tokens_hbm, gate_hbm, up_hbm, down_hbm,
    out_ref,
    tokens_ref, sendz, gathered, unpack, gate_send, gate_recv, w_gate, w_up, w_down, spare, hidden,
    r_send, own_sum, r_recv, home_send, home_recv, mixed, sq_send, sq_recv,
    tok_sem, w_sem, gate_ss, gate_rs, z_ss, z_rs, x_ss, x_rs, t_ss, t_rs, u_ss, u_rs, v_ss, v_rs,
    r_ss, r_rs, h_ss, h_rs, q_ss, q_rs,
):
    Q, S, R = group_count, span, rows
    N = Q * S
    RC = R // 2
    top, tok = routes_ref.shape
    width = tokens_ref.shape[1]
    H = out_ref.shape[1]
    L, _, F = gate_hbm.shape
    LF = L * F
    group_width = S * L
    lanes = gate_send.shape[-1]
    me = lax.axis_index("ep")
    c = lax.axis_index("tp")
    q, s = me // S, lax.rem(me, S)
    if Q == 4:
        middle = (q + 1) // 2 % 2
        place, order = [0, 3 - middle, 1, 2 + middle], [3 - 2 * middle, 2 + middle, 1 + middle]
    else:
        place, order = list(range(Q)), list(range(1, Q))
    pair = 2 if S % 2 == 0 else 1
    rows_at_once = pair * RC

    def at(ep, tp=None):
        return {"ep": ep, "tp": c if tp is None else tp}

    def remote(src, dst, ss, rs, dev):
        return pltpu.make_async_remote_copy(
            src_ref=src, dst_ref=dst, send_sem=ss, recv_sem=rs, device_id=dev, device_id_type=MESH
        )

    def chunk(k):
        return pl.ds(k * RC, RC)

    tok_copy = pltpu.make_async_copy(tokens_hbm, tokens_ref, tok_sem)
    tok_copy.start()

    barrier = pltpu.get_barrier_semaphore()
    loop(1, N, lambda p: pl.semaphore_signal(
        barrier, inc=1, device_id=at(lax.rem(me + p, N)), device_id_type=MESH))
    pl.semaphore_signal(barrier, inc=1, device_id=at(me, 1 - c), device_id_type=MESH)

    own_cols = pl.ds(pl.multiple_of(c * H, H), H)
    other_cols = pl.ds(pl.multiple_of((1 - c) * H, H), H)
    weights = []
    for n, (src, dst) in enumerate(((gate_hbm, w_gate), (up_hbm, w_up))):
        for e in range(L):
            weights.append(pltpu.make_async_copy(src.at[e], dst.at[e], w_sem.at[n, e]))
    for e in range(L):
        weights.append(pltpu.make_async_copy(
            down_hbm.at[e, :, own_cols], w_down.at[0, pl.ds(e * F, F)], w_sem.at[2, e]))
    away = [
        pltpu.make_async_copy(down_hbm.at[e, :, other_cols], spare.at[pl.ds(e * F, F)], w_sem.at[3, e]) for e in range(L)
    ]

    first = routes_ref[0:1, :]
    row_group = lax.broadcasted_iota(jnp.int32, (16, tok), 0)
    groups = jnp.full((16, tok), -1, jnp.int32)
    for d in range(Q):
        groups = jnp.where(row_group == d, partner(q, d, Q)[0], groups)
    member = (groups >= 0) & (first >= groups * group_width) & (first < (groups + 1) * group_width)
    earlier = lax.broadcasted_iota(jnp.int32, (tok, tok), 0) < lax.broadcasted_iota(jnp.int32, (tok, tok), 1)
    rank = jnp.dot(
        jnp.where(member, 1.0, 0.0).astype(BF16), jnp.where(earlier, 1.0, 0.0).astype(BF16),
        preferred_element_type=F32,
    ).astype(jnp.int32)
    slots = lax.broadcasted_iota(jnp.int32, (lanes, tok), 0)
    picks = []
    for d in range(Q):
        low = partner(q, d, Q)[0] * group_width
        inside = (first >= low) & (first < low + group_width)
        picks.append(jnp.where((rank[d:d + 1, :] == slots) & inside, 1.0, 0.0))

    tok_copy.wait()
    for copy in away + weights:
        copy.start()
    floats = tokens_ref[...].astype(F32)
    inv = lax.rsqrt(jnp.mean(floats * floats, axis=-1, keepdims=True) + EPS)
    normed = (tokens_ref[...].astype(F32) * inv * in_gain_ref[...]).astype(BF16)
    for d in range(Q):
        pick = jnp.where(c == 0, picks[d][:RC], picks[d][RC:R]).astype(BF16)
        block = jnp.dot(pick, normed, preferred_element_type=F32).astype(BF16)
        if d == 0:
            gathered[0, c, 0] = block
        else:
            sendz[d] = block

    pl.semaphore_wait(barrier, N)

    def z_copy(d):
        return remote(sendz.at[d], gathered.at[d, c, 0], z_ss.at[d], z_rs.at[d], at(partner(q, d, Q)[0] * S + s))

    def x_copy(d, e):
        return remote(
            gathered.at[d, c, 0], gathered.at[d, c, e], x_ss.at[d, e], x_rs.at[d, e], at(q * S + lax.rem(s + e, S)))

    def t_copy(d, e):
        block = gathered.at[d, c, e]
        return remote(block, block, t_ss.at[d, e], t_rs.at[d, e], at(me, 1 - c))

    def gate_copy(d, e):
        return remote(
            gate_send.at[d, lax.rem(s + e, S)], gate_recv.at[d, e], gate_ss.at[d, e], gate_rs.at[d, e],
            at(partner(q, d, Q)[0] * S + lax.rem(s + e, S)),
        )

    def u_copy():
        return remote(spare, w_down.at[1], u_ss, u_rs, at(me, 1 - c))

    def v_copy(d, k):
        return remote(hidden.at[d, k, 0], hidden.at[d, k, 1], v_ss.at[d, k], v_rs.at[d, k], at(me, 1 - c))

    def r_copy(d, e, k):
        return remote(
            r_send.at[d, k, e], r_recv.at[d, k, e], r_ss.at[d, e, k], r_rs.at[d, e, k],
            at(q * S + lax.rem(s + S - e, S)),
        )

    def h_copy(d, k):
        return remote(
            home_send.at[d, k], home_recv.at[d, k], h_ss.at[d, k], h_rs.at[d, k], at(partner(q, d, Q)[1] * S + s))

    def forward(d):
        loop(1, S, lambda e: x_copy(d, e).start())
        t_copy(d, 0).start()

    forward(0)
    for d in order:
        z_copy(d).start()
    for copy in away:
        copy.wait()
    u_copy().start()

    for d in range(Q):
        base = partner(q, d, Q)[0] * group_width
        ids = base + lax.broadcasted_iota(jnp.int32, (-(-group_width // 8) * 8, tok), 0)
        dense = jnp.zeros(ids.shape, F32)
        for k in range(top):
            dense += jnp.where(routes_ref[k:k + 1, :] == ids, probs_ref[k:k + 1, :], 0.0)
        lines = lax.dot_general(
            dense, picks[d], (((1,), (1,)), ((), ())),
            precision=lax.Precision.HIGHEST, preferred_element_type=F32,
        )
        for i in range(S):
            gate_send[d, i] = lines[i * L:(i + 1) * L]
    gate_recv[0, 0] = gate_send[0, s]
    for d in range(Q):
        loop(1 if d == 0 else 0, S, lambda e: gate_copy(d, e).start())

    for d in range(Q):
        for k in range(2):
            unpack[d, k] = picks[d][k * RC:(k + 1) * RC].T.astype(BF16)
    for copy in weights:
        copy.wait()

    row, lane = (lax.broadcasted_iota(jnp.int32, (RC, lanes), i) for i in (0, 1))

    def up_projection(d, k, n):
        base = n * pair
        tokens = gathered[d, k, pl.ds(base, pair)].reshape(rows_at_once, width)
        at_rows = pl.ds(n * rows_at_once, rows_at_once)
        for j in range(L):
            gate = jnp.dot(tokens, w_gate[j], preferred_element_type=F32)
            up = jnp.dot(tokens, w_up[j], preferred_element_type=F32)
            scale = jnp.concatenate([
                jnp.sum(jnp.where(row + k * RC == lane, gate_recv[d, base + b, pl.ds(j, 1), :], 0.0), axis=1, keepdims=True)
                for b in range(pair)
            ], axis=0)
            act = gate / (1.0 + jnp.exp(-gate)) * up
            hidden[d, k, 0, at_rows, j * F:(j + 1) * F] = (act * scale).astype(BF16)

    def down_projection(d, k, n, ready):
        at_rows = pl.ds(n * rows_at_once, rows_at_once)
        part = jnp.dot(hidden[d, k, 0, at_rows], w_down[0], preferred_element_type=F32)
        ready()
        return part + jnp.dot(hidden[d, k, 1, at_rows], w_down[1], preferred_element_type=F32)

    down_ready = []

    def step_a(p, k):
        d = place[p]

        @pl.when(c == k)
        def _():
            z_copy(d).wait_recv()
            forward(d)

    def step_b(p, k):
        d = place[p]

        def one(e):
            x_copy(d, e).wait_recv()
            t_copy(d, e).start()
        pl.when(c == k)(lambda: loop(1, S, one))

    def step_g(p, k):
        d = place[p]
        if k == 1:
            loop(1 if p == 0 else 0, S, lambda e: gate_copy(d, e).wait_recv())
        pl.when(c != k)(lambda: loop(0, S, lambda e: t_copy(d, e).wait_recv()))
        if S == pair:
            up_projection(d, k, 0)
        else:
            lax.fori_loop(0, S // pair, lambda n, carry: (up_projection(d, k, n), carry)[1], 0)
        v_copy(d, k).start()

    def step_d(p, k):
        d = place[p]
        if not down_ready:
            u_copy().wait_recv()
            down_ready.append(True)
        out = down_projection(d, k, 0, v_copy(d, k).wait_recv)
        for e in range(1, pair):
            r_send[d, k, e] = out[e * RC:(e + 1) * RC].astype(BF16)
        own_sum[d, k] = out[:RC]
        if S > pair:
            def some(n, carry):
                out = down_projection(d, k, n, lambda: None)
                r_send[d, k, pl.ds(n * pair, pair)] = out.astype(BF16).reshape(pair, RC, H)
                return carry
            lax.fori_loop(1, S // pair, some, 0)
        loop(1, S, lambda e: r_copy(d, e, k).start())

    def step_f(p, k):
        d = place[p]

        def one(e, total):
            r_copy(d, e, k).wait_recv()
            return total + r_recv[d, k, e].astype(F32)
        total = own_sum[d, k]
        if S <= 8:
            for e in range(1, S):
                total = one(e, total)
        else:
            total = lax.fori_loop(1, S, one, total)
        if p == 0:
            home_recv[0, k] = total.astype(BF16)
        else:
            home_send[d, k] = total.astype(BF16)
            h_copy(d, k).start()

    def step_m(p, k):
        d = place[p]
        if p > 0:
            h_copy(d, k).wait_recv()
        term = jnp.dot(unpack[d, k], home_recv[d, k], preferred_element_type=F32)
        mixed[...] = term if (p, k) == (0, 1) else mixed[...] + term

    actions = {"A": step_a, "B": step_b, "G": step_g, "D": step_d, "F": step_f, "M": step_m}

    steps = STEPS
    if Q != 4:
        units = [f"{p}{k}" for p in range(Q) for k in (1, 0)]
        steps = ["A" + u for u in units[2:]] + [x + u for x in "BGDFM" for u in units]
    for step in steps:
        actions[step[0]](*(int(i) for i in step[1:]))

    total = mixed[...]
    squares = jnp.sum(total * total, axis=1, keepdims=True)
    sq_send[...] = jnp.broadcast_to(squares, sq_send.shape)
    sq_copy = remote(sq_send, sq_recv, q_ss, q_rs, at(me, 1 - c))
    sq_copy.start()
    u_copy().wait_send()
    for d in range(Q):
        loop(1 if d == 0 else 0, S, lambda e: gate_copy(d, e).wait_send())
        loop(0, S, lambda e: t_copy(d, e).wait_send())
        loop(1, S, lambda e: x_copy(d, e).wait_send())
        if d > 0:
            z_copy(d).wait_send()
        for k in range(2):
            v_copy(d, k).wait_send()
            if d > 0:
                h_copy(d, k).wait_send()
            loop(1, S, lambda e: r_copy(d, e, k).wait_send())
    sq_copy.wait()
    norm = lax.rsqrt((squares + sq_recv[:, 0:1]) / width + EPS)
    out_ref[...] = (total * norm * out_gain_ref[...]).astype(BF16)


def body(tokens, in_gain, routing, gate_prob, w_gate, w_up, w_down, out_gain):
    N = lax.axis_size("ep")
    L, D, F = w_gate.shape
    tok, top = routing.shape
    H = out_gain.shape[0]
    group_width = L * N // GROUPS
    cap = max(2, tok * top // (2 * group_width))
    R = min(tok, group_width * cap // top)
    R = -(-R // 16) * 16
    Q, S, K = GROUPS, N // GROUPS, 2
    RC = R // K
    lanes = -(-R // 128) * 128
    vmem = pl.BlockSpec(memory_space=pltpu.VMEM)
    hbm = pl.BlockSpec(memory_space=pl.ANY)
    dma = pltpu.SemaphoreType.DMA
    return pl.pallas_call(
        functools.partial(kernel, Q, S, R),
        out_shape=jax.ShapeDtypeStruct((tok, H), BF16),
        in_specs=[vmem] * 4 + [hbm] * 4,
        out_specs=vmem,
        scratch_shapes=[
            pltpu.VMEM((tok, D), BF16),
            pltpu.VMEM((Q, RC, D), BF16),
            pltpu.VMEM((Q, K, S, RC, D), BF16),
            pltpu.VMEM((Q, K, tok, RC), BF16),
            pltpu.VMEM((Q, S, L, lanes), F32),
            pltpu.VMEM((Q, S, L, lanes), F32),
            pltpu.VMEM((L, D, F), BF16),
            pltpu.VMEM((L, D, F), BF16),
            pltpu.VMEM((2, L * F, H), BF16),
            pltpu.VMEM((L * F, H), BF16),
            pltpu.VMEM((Q, K, 2, S * RC, L * F), BF16),
            pltpu.VMEM((Q, K, S, RC, H), BF16),
            pltpu.VMEM((Q, K, RC, H), F32),
            pltpu.VMEM((Q, K, S, RC, H), BF16),
            pltpu.VMEM((Q, K, RC, H), BF16),
            pltpu.VMEM((Q, K, RC, H), BF16),
            pltpu.VMEM((tok, H), F32),
            pltpu.VMEM((tok, 128), F32),
            pltpu.VMEM((tok, 128), F32),
            dma, dma((4, L)), dma((Q, S)), dma((Q, S)), dma((Q,)), dma((Q,)),
            dma((Q, S)), dma((Q, S)), dma((Q, S)), dma((Q, S)), dma, dma,
            dma((Q, K)), dma((Q, K)), dma((Q, S, K)), dma((Q, S, K)), dma((Q, K)), dma((Q, K)),
            dma, dma,
        ],
        compiler_params=pltpu.CompilerParams(
            collective_id=0, has_side_effects=True, vmem_limit_bytes=64 * 1000 * 1000
        ),
    )(routing.T, gate_prob.T, in_gain.reshape(1, D), out_gain.reshape(1, H), tokens, w_gate, w_up, w_down)


def solution(mesh):
    placed = (
        P(("grp", "ep"), None),
        P(),
        P(("grp", "ep"), None),
        P(("grp", "ep"), None),
        P("ep", None, "tp"),
        P("ep", None, "tp"),
        P("ep", "tp", None),
        P("tp"),
    )
    return jax.shard_map(
        body, mesh=mesh, in_specs=placed, out_specs=P(("grp", "ep"), "tp"), check_vma=False
    )
```

```python
import functools

import jax
import jax.numpy as jnp
from jax import lax
from jax.experimental import pallas as pl
from jax.experimental.pallas import tpu as pltpu
from jax.sharding import PartitionSpec as P

GROUPS = 4
EPS = 1e-06
MESH = pl.DeviceIdType.MESH
F32 = jnp.float32
BF16 = jnp.bfloat16

STEPS = (
    "A21", "A11", "A20", "A10", "B21", "G21", "B01", "B11", "A31", "D21", "B20", "G20",
    "B10", "B00", "A30", "G11", "B31", "D20", "D11", "F21", "G31", "G10", "B30", "D31",
    "F20", "G30", "F11", "D30", "G00", "F31", "D10", "D00", "G01", "F30", "D01", "F10",
    "M21", "M31", "M11", "F00", "M00", "M20", "F01", "M01", "M10", "M30",
)
PLACES = ((1, 2, 3), (2, 1, 3), (1, 2, 3), (1, 2, 3))
ORDERS = ((1, 2, 3), (2, 3, 1), (1, 2, 3), (1, 2, 3))
PARTS = 2


def loop(low, high, step):
    if high - low <= 8:
        for i in range(low, high):
            step(i)
    else:
        lax.fori_loop(low, high, lambda i, carry: (step(i), carry)[1], 0)


def partner(q, d, count):
    if count & (count - 1):
        return lax.rem(q + d, count), lax.rem(q + count - d, count)
    other, bit = 0, 1
    while bit < count:
        mine, theirs = (q // bit) % 2, (d // bit) % 2
        other = other + bit * (mine + theirs - 2 * mine * theirs)
        bit *= 2
    return other, other


def kernel(
    group_count, span, rows,
    routes_hbm, probs_hbm, in_gain_hbm, out_gain_hbm, tokens_hbm, gate_hbm, up_hbm, down_hbm,
    out_ref,
    routes_ref, probs_ref, in_gain_ref, out_gain_ref, tokens_ref, sendz, gathered, unpack, gate_send, gate_recv, w_gate, w_up, w_down, spare, hidden,
    r_send, own_sum, r_recv, home_send, home_recv, mixed, sq_send, sq_recv,
    tok_sem, w_sem, gate_ss, gate_rs, z_ss, z_rs, x_ss, x_rs, t_ss, t_rs, u_ss, u_rs, v_ss, v_rs,
    r_ss, r_rs, h_ss, h_rs, q_ss, q_rs,
):
    Q, S, R = group_count, span, rows
    N = Q * S
    RC = R // 2
    top, tok = routes_ref.shape
    width = tokens_ref.shape[1]
    H = out_ref.shape[1]
    L, _, F = gate_hbm.shape
    W = width // PARTS
    group_width = S * L
    lanes = gate_send.shape[-1]
    me = lax.axis_index("ep")
    c = lax.axis_index("tp")
    q, s = me // S, lax.rem(me, S)
    if Q == 4:
        digit = (1 + 3 * (q % 2)) * (1 + 15 * (q // 2))

        def look_up(table):
            return [sum(row[i] * 4 ** z for z, row in enumerate(table)) // digit % 4 for i in range(3)]
        place, order = [0] + look_up(PLACES), look_up(ORDERS)
    else:
        place, order = list(range(Q)), list(range(1, Q))
    pair = 2 if S % 2 == 0 else 1
    rows_at_once = pair * RC

    def at(ep, tp=None):
        return {"ep": ep, "tp": c if tp is None else tp}

    def remote(src, dst, ss, rs, dev):
        return pltpu.make_async_remote_copy(
            src_ref=src, dst_ref=dst, send_sem=ss, recv_sem=rs, device_id=dev, device_id_type=MESH
        )

    def chunk(k):
        return pl.ds(k * RC, RC)

    small = [
        pltpu.make_async_copy(src, dst, tok_sem.at[i]) for i, (src, dst) in enumerate((
            (routes_hbm, routes_ref), (in_gain_hbm, in_gain_ref), (probs_hbm, probs_ref), (out_gain_hbm, out_gain_ref)))
    ]
    tok_copy = pltpu.make_async_copy(tokens_hbm, tokens_ref, tok_sem.at[4])
    small[0].start()
    tok_copy.start()
    for copy in small[1:]:
        copy.start()

    barrier = pltpu.get_barrier_semaphore()
    loop(1, N, lambda p: pl.semaphore_signal(
        barrier, inc=1, device_id=at(lax.rem(me + p, N)), device_id_type=MESH))
    pl.semaphore_signal(barrier, inc=1, device_id=at(me, 1 - c), device_id_type=MESH)

    own_cols = pl.ds(pl.multiple_of(c * H, H), H)
    other_cols = pl.ds(pl.multiple_of((1 - c) * H, H), H)
    weights = []
    for n, (src, dst) in enumerate(((gate_hbm, w_gate), (up_hbm, w_up))):
        for e in range(L):
            weights.append(pltpu.make_async_copy(src.at[e], dst.at[e], w_sem.at[n, e]))
    for e in range(L):
        weights.append(pltpu.make_async_copy(
            down_hbm.at[e, :, own_cols], w_down.at[0, pl.ds(e * F, F)], w_sem.at[2, e]))
    away = [
        pltpu.make_async_copy(down_hbm.at[e, :, other_cols], spare.at[pl.ds(e * F, F)], w_sem.at[3, e]) for e in range(L)
    ]

    small[0].wait()
    first = routes_ref[0:1, :]
    row_group = lax.broadcasted_iota(jnp.int32, (16, tok), 0)
    groups = jnp.full((16, tok), -1, jnp.int32)
    for d in range(Q):
        groups = jnp.where(row_group == d, partner(q, d, Q)[0], groups)
    member = (groups >= 0) & (first >= groups * group_width) & (first < (groups + 1) * group_width)
    earlier = lax.broadcasted_iota(jnp.int32, (tok, tok), 0) < lax.broadcasted_iota(jnp.int32, (tok, tok), 1)
    rank = jnp.dot(
        jnp.where(member, 1.0, 0.0).astype(BF16), jnp.where(earlier, 1.0, 0.0).astype(BF16),
        preferred_element_type=F32,
    ).astype(jnp.int32)
    slots = lax.broadcasted_iota(jnp.int32, (lanes, tok), 0)
    picks = []
    for d in range(Q):
        low = partner(q, d, Q)[0] * group_width
        inside = (first >= low) & (first < low + group_width)
        picks.append(jnp.where((rank[d:d + 1, :] == slots) & inside, 1.0, 0.0))

    tok_copy.wait()
    small[1].wait()
    for copy in away + weights:
        copy.start()
    floats = tokens_ref[...].astype(F32)
    inv = lax.rsqrt(jnp.mean(floats * floats, axis=-1, keepdims=True) + EPS)
    normed = (tokens_ref[...].astype(F32) * inv * in_gain_ref[...]).astype(BF16)
    for d in range(Q):
        pick = jnp.where(c == 0, picks[d][:RC], picks[d][RC:R]).astype(BF16)
        block = jnp.dot(pick, normed, preferred_element_type=F32).astype(BF16)
        for h in range(PARTS):
            if d == 0:
                gathered[0, c, h, 0] = block[:, h * W:(h + 1) * W]
            else:
                sendz[d, h] = block[:, h * W:(h + 1) * W]

    pl.semaphore_wait(barrier, N)

    def z_copy(d, h):
        return remote(
            sendz.at[d, h], gathered.at[d, c, h, 0], z_ss.at[d, h], z_rs.at[d, h], at(partner(q, d, Q)[0] * S + s))

    def x_copy(d, e, h):
        return remote(
            gathered.at[d, c, h, 0], gathered.at[d, c, h, e], x_ss.at[d, e, h], x_rs.at[d, e, h],
            at(q * S + lax.rem(s + e, S)),
        )

    def t_copy(d, e, h):
        block = gathered.at[d, c, h, e]
        return remote(block, block, t_ss.at[d, e, h], t_rs.at[d, e, h], at(me, 1 - c))

    def gate_copy(d, e):
        return remote(
            gate_send.at[d, lax.rem(s + e, S)], gate_recv.at[d, e], gate_ss.at[d, e], gate_rs.at[d, e],
            at(partner(q, d, Q)[0] * S + lax.rem(s + e, S)),
        )

    def u_copy():
        return remote(spare, w_down.at[1], u_ss, u_rs, at(me, 1 - c))

    def v_copy(d, k):
        return remote(hidden.at[d, k, 0], hidden.at[d, k, 1], v_ss.at[d, k], v_rs.at[d, k], at(me, 1 - c))

    def r_copy(d, e, k):
        return remote(
            r_send.at[d, k, e], r_recv.at[d, k, e], r_ss.at[d, e, k], r_rs.at[d, e, k],
            at(q * S + lax.rem(s + S - e, S)),
        )

    def h_copy(d, k):
        return remote(
            home_send.at[d, k], home_recv.at[d, k], h_ss.at[d, k], h_rs.at[d, k], at(partner(q, d, Q)[1] * S + s))

    def forward(d, h):
        loop(1, S, lambda e: x_copy(d, e, h).start())
        t_copy(d, 0, h).start()

    for h in range(PARTS):
        forward(0, h)
    for d in order:
        for h in range(PARTS):
            z_copy(d, h).start()
    for copy in away:
        copy.wait()
    u_copy().start()

    small[2].wait()
    small[3].wait()
    for d in range(Q):
        base = partner(q, d, Q)[0] * group_width
        ids = base + lax.broadcasted_iota(jnp.int32, (-(-group_width // 8) * 8, tok), 0)
        dense = jnp.zeros(ids.shape, F32)
        for k in range(top):
            dense += jnp.where(routes_ref[k:k + 1, :] == ids, probs_ref[k:k + 1, :], 0.0)
        lines = lax.dot_general(
            dense, picks[d], (((1,), (1,)), ((), ())),
            precision=lax.Precision.HIGHEST, preferred_element_type=F32,
        )
        for i in range(S):
            gate_send[d, i] = lines[i * L:(i + 1) * L]
    gate_recv[0, 0] = gate_send[0, s]
    for d in range(Q):
        loop(1 if d == 0 else 0, S, lambda e: gate_copy(d, e).start())

    for d in range(Q):
        for k in range(2):
            unpack[d, k] = picks[d][k * RC:(k + 1) * RC].T.astype(BF16)
    for copy in weights:
        copy.wait()

    row, lane = (lax.broadcasted_iota(jnp.int32, (RC, lanes), i) for i in (0, 1))

    def up_projection(d, k, n):
        base = n * pair
        tokens = jnp.concatenate(
            [gathered[d, k, h, pl.ds(base, pair)].reshape(rows_at_once, W) for h in range(PARTS)], axis=1)
        at_rows = pl.ds(n * rows_at_once, rows_at_once)
        for j in range(L):
            gate = jnp.dot(tokens, w_gate[j], preferred_element_type=F32)
            up = jnp.dot(tokens, w_up[j], preferred_element_type=F32)
            scale = jnp.concatenate([
                jnp.sum(jnp.where(row + k * RC == lane, gate_recv[d, base + b, pl.ds(j, 1), :], 0.0), axis=1, keepdims=True)
                for b in range(pair)
            ], axis=0)
            act = gate / (1.0 + jnp.exp(-gate)) * up
            hidden[d, k, 0, at_rows, j * F:(j + 1) * F] = (act * scale).astype(BF16)

    def down_projection(d, k, n, ready):
        at_rows = pl.ds(n * rows_at_once, rows_at_once)
        part = jnp.dot(hidden[d, k, 0, at_rows], w_down[0], preferred_element_type=F32)
        ready()
        return part + jnp.dot(hidden[d, k, 1, at_rows], w_down[1], preferred_element_type=F32)

    down_ready, gates_ready, mixed_ready = [], [], []

    def step_a(p, k):
        d = place[p]

        @pl.when(c == k)
        def _():
            for h in range(PARTS):
                z_copy(d, h).wait_recv()
                forward(d, h)

    def step_b(p, k):
        d = place[p]

        def one(e):
            for h in range(PARTS):
                x_copy(d, e, h).wait_recv()
                t_copy(d, e, h).start()
        pl.when(c == k)(lambda: loop(1, S, one))

    def step_g(p, k):
        d = place[p]
        if p not in gates_ready:
            loop(1 if p == 0 else 0, S, lambda e: gate_copy(d, e).wait_recv())
            gates_ready.append(p)


        def arrived(e):
            for h in range(PARTS):
                t_copy(d, e, h).wait_recv()
        pl.when(c != k)(lambda: loop(0, S, arrived))
        if S == pair:
            up_projection(d, k, 0)
        else:
            lax.fori_loop(0, S // pair, lambda n, carry: (up_projection(d, k, n), carry)[1], 0)
        v_copy(d, k).start()

    def step_d(p, k):
        d = place[p]
        if not down_ready:
            u_copy().wait_recv()
            down_ready.append(True)
        out = down_projection(d, k, 0, v_copy(d, k).wait_recv)
        for e in range(1, pair):
            r_send[d, k, e] = out[e * RC:(e + 1) * RC].astype(BF16)
        own_sum[d, k] = out[:RC]
        if S > pair:
            def some(n, carry):
                out = down_projection(d, k, n, lambda: None)
                r_send[d, k, pl.ds(n * pair, pair)] = out.astype(BF16).reshape(pair, RC, H)
                return carry
            lax.fori_loop(1, S // pair, some, 0)
        loop(1, S, lambda e: r_copy(d, e, k).start())

    def step_f(p, k):
        d = place[p]

        def one(e, total):
            r_copy(d, e, k).wait_recv()
            return total + r_recv[d, k, e].astype(F32)
        total = own_sum[d, k]
        if S <= 8:
            for e in range(1, S):
                total = one(e, total)
        else:
            total = lax.fori_loop(1, S, one, total)
        if p == 0:
            home_recv[0, k] = total.astype(BF16)
        else:
            home_send[d, k] = total.astype(BF16)
            h_copy(d, k).start()

    def step_m(p, k):
        d = place[p]
        if p > 0:
            h_copy(d, k).wait_recv()
        term = jnp.dot(unpack[d, k], home_recv[d, k], preferred_element_type=F32)
        mixed[...] = mixed[...] + term if mixed_ready else term
        mixed_ready.append(True)

    actions = {"A": step_a, "B": step_b, "G": step_g, "D": step_d, "F": step_f, "M": step_m}

    steps = STEPS
    if Q != 4:
        units = [f"{p}{k}" for p in range(Q) for k in (1, 0)]
        steps = ["A" + u for u in units[2:]] + [x + u for x in "BGDFM" for u in units]
    for step in steps:
        actions[step[0]](*(int(i) for i in step[1:]))

    total = mixed[...]
    squares = jnp.sum(total * total, axis=1, keepdims=True)
    sq_send[...] = jnp.broadcast_to(squares, sq_send.shape)
    sq_copy = remote(sq_send, sq_recv, q_ss, q_rs, at(me, 1 - c))
    sq_copy.start()
    u_copy().wait_send()
    for d in range(Q):
        loop(1 if d == 0 else 0, S, lambda e: gate_copy(d, e).wait_send())
        for h in range(PARTS):
            loop(0, S, lambda e: t_copy(d, e, h).wait_send())
            loop(1, S, lambda e: x_copy(d, e, h).wait_send())
            if d > 0:
                z_copy(d, h).wait_send()
        for k in range(2):
            v_copy(d, k).wait_send()
            if d > 0:
                h_copy(d, k).wait_send()
            loop(1, S, lambda e: r_copy(d, e, k).wait_send())
    sq_copy.wait()
    norm = lax.rsqrt((squares + sq_recv[:, 0:1]) / width + EPS)
    out_ref[...] = (total * norm * out_gain_ref[...]).astype(BF16)


def body(tokens, in_gain, routing, gate_prob, w_gate, w_up, w_down, out_gain):
    N = lax.axis_size("ep")
    L, D, F = w_gate.shape
    tok, top = routing.shape
    H = out_gain.shape[0]
    group_width = L * N // GROUPS
    cap = max(2, tok * top // (2 * group_width))
    R = min(tok, group_width * cap // top)
    R = -(-R // 16) * 16
    Q, S, K = GROUPS, N // GROUPS, 2
    RC = R // K
    lanes = -(-R // 128) * 128
    vmem = pl.BlockSpec(memory_space=pltpu.VMEM)
    hbm = pl.BlockSpec(memory_space=pl.ANY)
    dma = pltpu.SemaphoreType.DMA
    return pl.pallas_call(
        functools.partial(kernel, Q, S, R),
        out_shape=jax.ShapeDtypeStruct((tok, H), BF16),
        in_specs=[hbm] * 8,
        out_specs=vmem,
        scratch_shapes=[
            pltpu.VMEM((top, tok), jnp.int32),
            pltpu.VMEM((top, tok), F32),
            pltpu.VMEM((1, D), F32),
            pltpu.VMEM((1, H), F32),
            pltpu.VMEM((tok, D), BF16),
            pltpu.VMEM((Q, PARTS, RC, D // PARTS), BF16),
            pltpu.VMEM((Q, K, PARTS, S, RC, D // PARTS), BF16),
            pltpu.VMEM((Q, K, tok, RC), BF16),
            pltpu.VMEM((Q, S, L, lanes), F32),
            pltpu.VMEM((Q, S, L, lanes), F32),
            pltpu.VMEM((L, D, F), BF16),
            pltpu.VMEM((L, D, F), BF16),
            pltpu.VMEM((2, L * F, H), BF16),
            pltpu.VMEM((L * F, H), BF16),
            pltpu.VMEM((Q, K, 2, S * RC, L * F), BF16),
            pltpu.VMEM((Q, K, S, RC, H), BF16),
            pltpu.VMEM((Q, K, RC, H), F32),
            pltpu.VMEM((Q, K, S, RC, H), BF16),
            pltpu.VMEM((Q, K, RC, H), BF16),
            pltpu.VMEM((Q, K, RC, H), BF16),
            pltpu.VMEM((tok, H), F32),
            pltpu.VMEM((tok, 128), F32),
            pltpu.VMEM((tok, 128), F32),
            dma((5,)), dma((4, L)), dma((Q, S)), dma((Q, S)), dma((Q, PARTS)), dma((Q, PARTS)),
            dma((Q, S, PARTS)), dma((Q, S, PARTS)), dma((Q, S, PARTS)), dma((Q, S, PARTS)), dma, dma,
            dma((Q, K)), dma((Q, K)), dma((Q, S, K)), dma((Q, S, K)), dma((Q, K)), dma((Q, K)),
            dma, dma,
        ],
        compiler_params=pltpu.CompilerParams(
            collective_id=0, has_side_effects=True, vmem_limit_bytes=64 * 1000 * 1000
        ),
    )(routing.T, gate_prob.T, in_gain.reshape(1, D), out_gain.reshape(1, H), tokens, w_gate, w_up, w_down)


def solution(mesh):
    placed = (
        P(("grp", "ep"), None),
        P(),
        P(("grp", "ep"), None),
        P(("grp", "ep"), None),
        P("ep", None, "tp"),
        P("ep", None, "tp"),
        P("ep", "tp", None),
        P("tp"),
    )
    return jax.shard_map(
        body, mesh=mesh, in_specs=placed, out_specs=P(("grp", "ep"), "tp"), check_vma=False
    )
```

```python
import functools

import jax
import jax.numpy as jnp
from jax import lax
from jax.experimental import pallas as pl
from jax.experimental.pallas import tpu as pltpu
from jax.sharding import PartitionSpec as P

GROUPS = 4
EPS = 1e-06
MESH = pl.DeviceIdType.MESH
F32 = jnp.float32
BF16 = jnp.bfloat16

STEPS = (
    "B00", "A11", "A31", "B11", "G00", "B01", "A10", "A30", "G11", "A21", "B10", "D11",
    "G10", "B30", "D10", "B31", "A20", "B21", "G30", "F11", "G21", "D30", "D21", "G31",
    "B20", "F10", "D31", "G20", "F30", "D20", "F21", "G01", "F31", "D00", "D01", "F20",
    "M10", "M30", "M21", "F00", "M00", "M11", "F01", "M01", "M20", "M31",
)
PLACES = ((3, 2, 1), (2, 3, 1), (2, 3, 1), (3, 2, 1))
ORDERS = ((3, 2, 1), (2, 1, 3), (2, 3, 1), (3, 2, 1))
PARTS = 2


def loop(low, high, step):
    if high - low <= 8:
        for i in range(low, high):
            step(i)
    else:
        lax.fori_loop(low, high, lambda i, carry: (step(i), carry)[1], 0)


def partner(q, d, count):
    if count & (count - 1):
        return lax.rem(q + d, count), lax.rem(q + count - d, count)
    other, bit = 0, 1
    while bit < count:
        mine, theirs = (q // bit) % 2, (d // bit) % 2
        other = other + bit * (mine + theirs - 2 * mine * theirs)
        bit *= 2
    return other, other


def kernel(
    group_count, span, rows,
    routes_hbm, probs_hbm, in_gain_hbm, out_gain_hbm, tokens_hbm, gate_hbm, up_hbm, down_hbm,
    out_ref,
    routes_ref, probs_ref, in_gain_ref, out_gain_ref, tokens_ref, sendz, gathered, unpack, gate_send, gate_recv, w_gate, w_up, w_down, spare, hidden,
    r_send, own_sum, r_recv, home_send, home_recv, mixed, sq_send, sq_recv,
    tok_sem, w_sem, gate_ss, gate_rs, z_ss, z_rs, x_ss, x_rs, t_ss, t_rs, u_ss, u_rs, v_ss, v_rs,
    r_ss, r_rs, h_ss, h_rs, q_ss, q_rs,
):
    Q, S, R = group_count, span, rows
    N = Q * S
    RC = R // 2
    top, tok = routes_ref.shape
    width = tokens_ref.shape[1]
    H = out_ref.shape[1]
    L, _, F = gate_hbm.shape
    W = width // PARTS
    group_width = S * L
    lanes = gate_send.shape[-1]
    me = lax.axis_index("ep")
    c = lax.axis_index("tp")
    q, s = me // S, lax.rem(me, S)
    if Q == 4:
        digit = (1 + 3 * (q % 2)) * (1 + 15 * (q // 2))

        def look_up(table):
            return [sum(row[i] * 4 ** z for z, row in enumerate(table)) // digit % 4 for i in range(3)]
        place, order = [0] + look_up(PLACES), look_up(ORDERS)
    else:
        place, order = list(range(Q)), list(range(1, Q))
    pair = 2 if S % 2 == 0 else 1
    rows_at_once = pair * RC

    def at(ep, tp=None):
        return {"ep": ep, "tp": c if tp is None else tp}

    def remote(src, dst, ss, rs, dev):
        return pltpu.make_async_remote_copy(
            src_ref=src, dst_ref=dst, send_sem=ss, recv_sem=rs, device_id=dev, device_id_type=MESH
        )

    def chunk(k):
        return pl.ds(k * RC, RC)

    small = [
        pltpu.make_async_copy(src, dst, tok_sem.at[i]) for i, (src, dst) in enumerate((
            (routes_hbm, routes_ref), (in_gain_hbm, in_gain_ref), (probs_hbm, probs_ref), (out_gain_hbm, out_gain_ref)))
    ]
    tok_copy = pltpu.make_async_copy(tokens_hbm, tokens_ref, tok_sem.at[4])
    small[0].start()
    tok_copy.start()
    for copy in small[1:]:
        copy.start()

    barrier = pltpu.get_barrier_semaphore()
    loop(1, N, lambda p: pl.semaphore_signal(
        barrier, inc=1, device_id=at(lax.rem(me + p, N)), device_id_type=MESH))
    pl.semaphore_signal(barrier, inc=1, device_id=at(me, 1 - c), device_id_type=MESH)

    own_cols = pl.ds(pl.multiple_of(c * H, H), H)
    other_cols = pl.ds(pl.multiple_of((1 - c) * H, H), H)
    weights = [
        pltpu.make_async_copy(gate_hbm, w_gate, w_sem.at[0]),
        pltpu.make_async_copy(up_hbm, w_up, w_sem.at[1]),
        pltpu.make_async_copy(down_hbm.at[:, :, own_cols], w_down.at[0], w_sem.at[2]),
    ]
    away = pltpu.make_async_copy(down_hbm.at[:, :, other_cols], spare, w_sem.at[3])

    small[0].wait()
    first = routes_ref[0:1, :]
    row_group = lax.broadcasted_iota(jnp.int32, (16, tok), 0)
    groups = jnp.full((16, tok), -1, jnp.int32)
    for d in range(Q):
        groups = jnp.where(row_group == d, partner(q, d, Q)[0], groups)
    member = (groups >= 0) & (first >= groups * group_width) & (first < (groups + 1) * group_width)
    earlier = lax.broadcasted_iota(jnp.int32, (tok, tok), 0) < lax.broadcasted_iota(jnp.int32, (tok, tok), 1)
    rank = jnp.dot(
        jnp.where(member, 1.0, 0.0).astype(BF16), jnp.where(earlier, 1.0, 0.0).astype(BF16),
        preferred_element_type=F32,
    ).astype(jnp.int32)
    slots = lax.broadcasted_iota(jnp.int32, (lanes, tok), 0)
    picks = []
    for d in range(Q):
        low = partner(q, d, Q)[0] * group_width
        inside = (first >= low) & (first < low + group_width)
        picks.append(jnp.where((rank[d:d + 1, :] == slots) & inside, 1.0, 0.0))

    tok_copy.wait()
    small[1].wait()
    for copy in [away] + weights:
        copy.start()
    floats = tokens_ref[...].astype(F32)
    inv = lax.rsqrt(jnp.mean(floats * floats, axis=-1, keepdims=True) + EPS)
    normed = (tokens_ref[...].astype(F32) * inv * in_gain_ref[...]).astype(BF16)
    for d in range(Q):
        pick = jnp.where(c == 0, picks[d][:RC], picks[d][RC:R]).astype(BF16)
        block = jnp.dot(pick, normed, preferred_element_type=F32).astype(BF16)
        for h in range(PARTS):
            if d == 0:
                gathered[0, c, h, 0] = block[:, h * W:(h + 1) * W]
            else:
                sendz[d - 1, h] = block[:, h * W:(h + 1) * W]

    pl.semaphore_wait(barrier, N)

    def z_copy(d, h):
        return remote(
            sendz.at[d - 1, h], gathered.at[d, c, h, 0], z_ss, z_rs.at[d - 1, h], at(partner(q, d, Q)[0] * S + s))

    def x_copy(d, e, h):
        return remote(
            gathered.at[d, c, h, 0], gathered.at[d, c, h, e], x_ss, x_rs.at[d, e - 1, h],
            at(q * S + lax.rem(s + e, S)),
        )

    def t_copy(d, e, h):
        block = gathered.at[d, c, h, e]
        return remote(block, block, t_ss, t_rs.at[d], at(me, 1 - c))

    def gate_copy(d, e, near):
        return remote(
            gate_send.at[d, lax.rem(s + e, S)], gate_recv.at[d, e], gate_ss.at[near], gate_rs.at[d],
            at(partner(q, d, Q)[0] * S + lax.rem(s + e, S)),
        )

    def u_copy():
        return remote(spare, w_down.at[1], u_ss, u_rs, at(me, 1 - c))

    def v_copy(d, k):
        return remote(hidden.at[d, k, 0], hidden.at[d, k, 1], v_ss, v_rs.at[d, k], at(me, 1 - c))

    def r_copy(d, e, k):
        return remote(
            r_send.at[d, k, e - 1], r_recv.at[d, k, e - 1], r_ss, r_rs.at[d, k],
            at(q * S + lax.rem(s + S - e, S)),
        )

    def h_copy(d, k):
        return remote(
            home_send.at[d - 1, k], home_recv.at[d, k], h_ss, h_rs.at[d - 1, k], at(partner(q, d, Q)[1] * S + s))

    def forward(d, h):
        loop(1, S, lambda e: x_copy(d, e, h).start())
        t_copy(d, 0, h).start()

    for h in range(PARTS):
        forward(0, h)
    for d in order:
        for h in range(PARTS):
            z_copy(d, h).start()
    away.wait()
    u_copy().start()

    small[2].wait()
    small[3].wait()
    for d in range(Q):
        base = partner(q, d, Q)[0] * group_width
        ids = base + lax.broadcasted_iota(jnp.int32, (-(-group_width // 8) * 8, tok), 0)
        dense = jnp.zeros(ids.shape, F32)
        for k in range(top):
            dense += jnp.where(routes_ref[k:k + 1, :] == ids, probs_ref[k:k + 1, :], 0.0)
        lines = lax.dot_general(
            dense, picks[d], (((1,), (1,)), ((), ())),
            precision=lax.Precision.HIGHEST, preferred_element_type=F32,
        )
        for i in range(S):
            gate_send[d, i] = lines[i * L:(i + 1) * L]
    gate_recv[0, 0] = gate_send[0, s]
    for d in range(Q):
        loop(1 if d == 0 else 0, S, lambda e: gate_copy(d, e, int(d == 0)).start())

    for d in range(Q):
        for k in range(2):
            unpack[d, k] = picks[d][k * RC:(k + 1) * RC].T.astype(BF16)
    for copy in weights:
        copy.wait()

    row, lane = (lax.broadcasted_iota(jnp.int32, (RC, lanes), i) for i in (0, 1))

    def up_projection(d, k, n):
        base = n * pair
        tokens = jnp.concatenate(
            [gathered[d, k, h, pl.ds(base, pair)].reshape(rows_at_once, W) for h in range(PARTS)], axis=1)
        at_rows = pl.ds(n * rows_at_once, rows_at_once)
        for j in range(L):
            gate = jnp.dot(tokens, w_gate[j], preferred_element_type=F32)
            up = jnp.dot(tokens, w_up[j], preferred_element_type=F32)
            scale = jnp.concatenate([
                jnp.sum(jnp.where(row + k * RC == lane, gate_recv[d, base + b, pl.ds(j, 1), :], 0.0), axis=1, keepdims=True)
                for b in range(pair)
            ], axis=0)
            act = gate / (1.0 + jnp.exp(-gate)) * up
            hidden[d, k, 0, at_rows, j * F:(j + 1) * F] = (act * scale).astype(BF16)

    def down_projection(d, k, n, ready):
        at_rows = pl.ds(n * rows_at_once, rows_at_once)
        part = jnp.dot(hidden[d, k, 0, at_rows], w_down[0].reshape(L * F, H), preferred_element_type=F32)
        ready()
        return part + jnp.dot(hidden[d, k, 1, at_rows], w_down[1].reshape(L * F, H), preferred_element_type=F32)

    def arrived(block, sem):
        remote(block, block, sem, sem, at(me, 1 - c)).wait_recv()

    def sent(block, sem):
        remote(block, block, sem, sem, at(me, 1 - c)).wait_send()

    down_ready, gates_ready, mixed_ready = [], [], []

    def step_a(p, k):
        d = place[p]

        @pl.when(c == k)
        def _():
            for h in range(PARTS):
                z_copy(d, h).wait_recv()
                forward(d, h)

    def step_b(p, k):
        d = place[p]

        def one(e):
            for h in range(PARTS):
                x_copy(d, e, h).wait_recv()
                t_copy(d, e, h).start()
        pl.when(c == k)(lambda: loop(1, S, one))

    def step_g(p, k):
        d = place[p]
        if p not in gates_ready:
            arrived(gate_recv.at[d, pl.ds(1, S - 1)] if p == 0 else gate_recv.at[d], gate_rs.at[d])
            gates_ready.append(p)

        pl.when(c != k)(lambda: arrived(gathered.at[d, 1 - c], t_rs.at[d]))
        if S == pair:
            up_projection(d, k, 0)
        else:
            lax.fori_loop(0, S // pair, lambda n, carry: (up_projection(d, k, n), carry)[1], 0)
        v_copy(d, k).start()

    def step_d(p, k):
        d = place[p]
        if not down_ready:
            u_copy().wait_recv()
            down_ready.append(True)
        out = down_projection(d, k, 0, v_copy(d, k).wait_recv)
        for e in range(1, pair):
            r_send[d, k, e - 1] = out[e * RC:(e + 1) * RC].astype(BF16)
        own_sum[d, k] = out[:RC]
        if S > pair:
            def some(n, carry):
                out = down_projection(d, k, n, lambda: None)
                r_send[d, k, pl.ds(n * pair - 1, pair)] = out.astype(BF16).reshape(pair, RC, H)
                return carry
            lax.fori_loop(1, S // pair, some, 0)
        loop(1, S, lambda e: r_copy(d, e, k).start())

    def step_f(p, k):
        d = place[p]

        arrived(r_recv.at[d, k], r_rs.at[d, k])
        total = own_sum[d, k]
        if S <= 8:
            for e in range(1, S):
                total = total + r_recv[d, k, e - 1].astype(F32)
        else:
            total = lax.fori_loop(1, S, lambda e, total: total + r_recv[d, k, e - 1].astype(F32), total)
        if p == 0:
            home_recv[0, k] = total.astype(BF16)
        else:
            home_send[d - 1, k] = total.astype(BF16)
            h_copy(d, k).start()

    def step_m(p, k):
        d = place[p]
        if p > 0:
            h_copy(d, k).wait_recv()
        term = jnp.dot(unpack[d, k], home_recv[d, k], preferred_element_type=F32)
        mixed[...] = mixed[...] + term if mixed_ready else term
        mixed_ready.append(True)

    actions = {"A": step_a, "B": step_b, "G": step_g, "D": step_d, "F": step_f, "M": step_m}

    steps = STEPS
    if Q != 4:
        units = [f"{p}{k}" for p in range(Q) for k in (1, 0)]
        steps = ["A" + u for u in units[2:]] + [x + u for x in "BGDFM" for u in units]
    for step in steps:
        actions[step[0]](*(int(i) for i in step[1:]))

    total = mixed[...]
    squares = jnp.sum(total * total, axis=1, keepdims=True)
    sq_send[...] = jnp.broadcast_to(squares, sq_send.shape)
    sq_copy = remote(sq_send, sq_recv, q_ss, q_rs, at(me, 1 - c))
    sq_copy.start()
    u_copy().wait_send()
    sent(gate_send.at[pl.ds(1, Q - 1)], gate_ss.at[0])
    sent(gate_send.at[0, pl.ds(1, S - 1)], gate_ss.at[1])
    sent(sendz, z_ss)
    sent(gathered.at[:, c, :, pl.ds(1, S - 1)], x_ss)
    sent(gathered.at[:, c], t_ss)
    sent(hidden.at[:, :, 0], v_ss)
    sent(r_send, r_ss)
    sent(home_send, h_ss)
    sq_copy.wait()
    norm = lax.rsqrt((squares + sq_recv[:, 0:1]) / width + EPS)
    out_ref[...] = (total * norm * out_gain_ref[...]).astype(BF16)


def body(tokens, in_gain, routing, gate_prob, w_gate, w_up, w_down, out_gain):
    N = lax.axis_size("ep")
    L, D, F = w_gate.shape
    tok, top = routing.shape
    H = out_gain.shape[0]
    group_width = L * N // GROUPS
    cap = max(2, tok * top // (2 * group_width))
    R = min(tok, group_width * cap // top)
    R = -(-R // 16) * 16
    Q, S, K = GROUPS, N // GROUPS, 2
    RC = R // K
    lanes = -(-R // 128) * 128
    vmem = pl.BlockSpec(memory_space=pltpu.VMEM)
    hbm = pl.BlockSpec(memory_space=pl.ANY)
    dma = pltpu.SemaphoreType.DMA
    return pl.pallas_call(
        functools.partial(kernel, Q, S, R),
        out_shape=pltpu.VMEM((tok, H), BF16),
        in_specs=[hbm] * 8,
        out_specs=vmem,
        scratch_shapes=[
            pltpu.VMEM((top, tok), jnp.int32),
            pltpu.VMEM((top, tok), F32),
            pltpu.VMEM((1, D), F32),
            pltpu.VMEM((1, H), F32),
            pltpu.VMEM((tok, D), BF16),
            pltpu.VMEM((Q - 1, PARTS, RC, D // PARTS), BF16),
            pltpu.VMEM((Q, K, PARTS, S, RC, D // PARTS), BF16),
            pltpu.VMEM((Q, K, tok, RC), BF16),
            pltpu.VMEM((Q, S, L, lanes), F32),
            pltpu.VMEM((Q, S, L, lanes), F32),
            pltpu.VMEM((L, D, F), BF16),
            pltpu.VMEM((L, D, F), BF16),
            pltpu.VMEM((2, L, F, H), BF16),
            pltpu.VMEM((L, F, H), BF16),
            pltpu.VMEM((Q, K, 2, S * RC, L * F), BF16),
            pltpu.VMEM((Q, K, S - 1, RC, H), BF16),
            pltpu.VMEM((Q, K, RC, H), F32),
            pltpu.VMEM((Q, K, S - 1, RC, H), BF16),
            pltpu.VMEM((Q - 1, K, RC, H), BF16),
            pltpu.VMEM((Q, K, RC, H), BF16),
            pltpu.VMEM((tok, H), F32),
            pltpu.VMEM((tok, 128), F32),
            pltpu.VMEM((tok, 128), F32),
            dma((5,)), dma((4,)), dma((2,)), dma((Q,)), dma, dma((Q - 1, PARTS)), dma, dma((Q, S - 1, PARTS)),
            dma, dma((Q,)), dma, dma, dma, dma((Q, K)), dma, dma((Q, K)), dma, dma((Q - 1, K)), dma, dma,
        ],
        compiler_params=pltpu.CompilerParams(
            collective_id=0, has_side_effects=True, vmem_limit_bytes=64 * 1000 * 1000
        ),
    )(routing.T, gate_prob.T, in_gain.reshape(1, D), out_gain.reshape(1, H), tokens, w_gate, w_up, w_down)


def solution(mesh):
    placed = (
        P(("grp", "ep"), None),
        P(),
        P(("grp", "ep"), None),
        P(("grp", "ep"), None),
        P("ep", None, "tp"),
        P("ep", None, "tp"),
        P("ep", "tp", None),
        P("tp"),
    )
    return jax.shard_map(
        body, mesh=mesh, in_specs=placed, out_specs=P(("grp", "ep"), "tp"), check_vma=False
    )
```

```python
import functools

import jax
import jax.numpy as jnp
from jax import lax
from jax.experimental import pallas as pl
from jax.experimental.pallas import tpu as pltpu
from jax.sharding import PartitionSpec as P

GROUPS = 4
EPS = 1e-06
MESH = pl.DeviceIdType.MESH
F32 = jnp.float32
BF16 = jnp.bfloat16

STEPS = (
    "A21", "B01", "A31", "B00", "A20", "B21", "G01", "A30", "G21", "G00", "A11", "B20",
    "D21", "G20", "B31", "B30", "A10", "G30", "B11", "D20", "D30", "F21", "G11", "G31",
    "B10", "D11", "F20", "D31", "G10", "F30", "D10", "F11", "F31", "D01", "D00", "F10",
    "M30", "M21", "F00", "M00", "M20", "M11", "F01", "M01", "M10", "M31",
)
PLACES = ((2, 3, 1), (3, 2, 1), (3, 2, 1), (2, 3, 1))
ORDERS = ((3, 2, 1), (1, 2, 3), (2, 3, 1), (3, 2, 1))
PARTS = 2


def loop(low, high, step):
    if high - low <= 8:
        for i in range(low, high):
            step(i)
    else:
        lax.fori_loop(low, high, lambda i, carry: (step(i), carry)[1], 0)


def partner(q, d, count):
    if count & (count - 1):
        return lax.rem(q + d, count), lax.rem(q + count - d, count)
    other, bit = 0, 1
    while bit < count:
        mine, theirs = (q // bit) % 2, (d // bit) % 2
        other = other + bit * (mine + theirs - 2 * mine * theirs)
        bit *= 2
    return other, other


def kernel(
    group_count, span, rows,
    routes_hbm, probs_hbm, in_gain_hbm, out_gain_hbm, tokens_hbm, gate_hbm, up_hbm, down_hbm,
    out_ref,
    routes_ref, probs_ref, in_gain_ref, out_gain_ref, tokens_ref, sendz, gathered, unpack, gate_send, gate_recv, w_gate, w_up, w_down, spare, hidden,
    r_send, own_sum, r_recv, home_send, home_recv, mixed, sq_send, sq_recv,
    tok_sem, w_sem, gate_ss, gate_rs, z_ss, z_rs, x_ss, x_rs, t_ss, t_rs, u_ss, u_rs, v_ss, v_rs,
    r_ss, r_rs, h_ss, h_rs, q_ss, q_rs,
):
    Q, S, R = group_count, span, rows
    N = Q * S
    RC = R // 2
    top, tok = routes_ref.shape
    width = tokens_ref.shape[1]
    H = out_ref.shape[1]
    L, _, F = gate_hbm.shape
    W = width // PARTS
    group_width = S * L
    lanes = gate_send.shape[-1]
    me = lax.axis_index("ep")
    c = lax.axis_index("tp")
    q, s = me // S, lax.rem(me, S)
    if Q == 4:
        digit = (1 + 3 * (q % 2)) * (1 + 15 * (q // 2))

        def look_up(table):
            return [sum(row[i] * 4 ** z for z, row in enumerate(table)) // digit % 4 for i in range(3)]
        place, order = [0] + look_up(PLACES), look_up(ORDERS)
    else:
        place, order = list(range(Q)), list(range(1, Q))
    pair = 2 if S % 2 == 0 else 1
    rows_at_once = pair * RC

    def at(ep, tp=None):
        return {"ep": ep, "tp": c if tp is None else tp}

    def remote(src, dst, ss, rs, dev):
        return pltpu.make_async_remote_copy(
            src_ref=src, dst_ref=dst, send_sem=ss, recv_sem=rs, device_id=dev, device_id_type=MESH
        )

    def chunk(k):
        return pl.ds(k * RC, RC)

    small = [
        pltpu.make_async_copy(src, dst, tok_sem.at[i]) for i, (src, dst) in enumerate((
            (routes_hbm, routes_ref), (in_gain_hbm, in_gain_ref), (probs_hbm, probs_ref), (out_gain_hbm, out_gain_ref)))
    ]
    tok_copy = pltpu.make_async_copy(tokens_hbm, tokens_ref, tok_sem.at[4])
    small[0].start()
    tok_copy.start()
    for copy in small[1:]:
        copy.start()

    barrier = pltpu.get_barrier_semaphore()
    loop(1, N, lambda p: pl.semaphore_signal(
        barrier, inc=1, device_id=at(lax.rem(me + p, N)), device_id_type=MESH))
    pl.semaphore_signal(barrier, inc=1, device_id=at(me, 1 - c), device_id_type=MESH)

    own_cols = pl.ds(pl.multiple_of(c * H, H), H)
    other_cols = pl.ds(pl.multiple_of((1 - c) * H, H), H)
    weights = [
        pltpu.make_async_copy(gate_hbm, w_gate, w_sem.at[0]),
        pltpu.make_async_copy(up_hbm, w_up, w_sem.at[1]),
        pltpu.make_async_copy(down_hbm.at[:, :, own_cols], w_down.at[0], w_sem.at[2]),
    ]
    away = pltpu.make_async_copy(down_hbm.at[:, :, other_cols], spare, w_sem.at[3])

    small[0].wait()
    first = routes_ref[0:1, :]
    row_group = lax.broadcasted_iota(jnp.int32, (16, tok), 0)
    groups = jnp.full((16, tok), -1, jnp.int32)
    for d in range(Q):
        groups = jnp.where(row_group == d, partner(q, d, Q)[0], groups)
    member = (groups >= 0) & (first >= groups * group_width) & (first < (groups + 1) * group_width)
    earlier = lax.broadcasted_iota(jnp.int32, (tok, tok), 0) < lax.broadcasted_iota(jnp.int32, (tok, tok), 1)
    rank = jnp.dot(
        jnp.where(member, 1.0, 0.0).astype(BF16), jnp.where(earlier, 1.0, 0.0).astype(BF16),
        preferred_element_type=F32,
    ).astype(jnp.int32)
    slots = lax.broadcasted_iota(jnp.int32, (lanes, tok), 0)
    picks = []
    for d in range(Q):
        low = partner(q, d, Q)[0] * group_width
        inside = (first >= low) & (first < low + group_width)
        picks.append(jnp.where((rank[d:d + 1, :] == slots) & inside, 1.0, 0.0))

    tok_copy.wait()
    small[1].wait()
    for copy in [away] + weights:
        copy.start()
    floats = tokens_ref[...].astype(F32)
    inv = lax.rsqrt(jnp.mean(floats * floats, axis=-1, keepdims=True) + EPS)
    normed = (tokens_ref[...].astype(F32) * inv * in_gain_ref[...]).astype(BF16)
    for d in range(Q):
        pick = jnp.where(c == 0, picks[d][:RC], picks[d][RC:R]).astype(BF16)
        block = jnp.dot(pick, normed, preferred_element_type=F32).astype(BF16)
        for h in range(PARTS):
            if d == 0:
                gathered[0, c, h, 0] = block[:, h * W:(h + 1) * W]
            else:
                sendz[d - 1, h] = block[:, h * W:(h + 1) * W]

    pl.semaphore_wait(barrier, N)

    def z_copy(d, h):
        return remote(
            sendz.at[d - 1, h], gathered.at[d, c, h, 0], z_ss, z_rs.at[d - 1, h], at(partner(q, d, Q)[0] * S + s))

    def x_copy(d, e, h):
        return remote(
            gathered.at[d, c, h, 0], gathered.at[d, c, h, e], x_ss, x_rs.at[d, e - 1, h],
            at(q * S + lax.rem(s + e, S)),
        )

    def t_copy(d, e, h):
        block = gathered.at[d, c, h, e]
        return remote(block, block, t_ss, t_rs.at[d], at(me, 1 - c))

    def gate_copy(d, e, near):
        return remote(
            gate_send.at[d, lax.rem(s + e, S)], gate_recv.at[d, e], gate_ss.at[near], gate_rs.at[d],
            at(partner(q, d, Q)[0] * S + lax.rem(s + e, S)),
        )

    def u_copy():
        return remote(spare, w_down.at[1], u_ss, u_rs, at(me, 1 - c))

    def v_copy(d, k):
        return remote(hidden.at[d, k, 0], hidden.at[d, k, 1], v_ss, v_rs.at[d, k], at(me, 1 - c))

    def r_copy(d, e, k):
        return remote(
            r_send.at[d, k, e - 1], r_recv.at[d, k, e - 1], r_ss, r_rs.at[d, k],
            at(q * S + lax.rem(s + S - e, S)),
        )

    def h_copy(d, k):
        return remote(
            home_send.at[d - 1, k], home_recv.at[d, k], h_ss, h_rs.at[d - 1, k], at(partner(q, d, Q)[1] * S + s))

    def forward(d, h):
        loop(1, S, lambda e: x_copy(d, e, h).start())
        t_copy(d, 0, h).start()

    for h in range(PARTS):
        forward(0, h)
    def leave(d):
        for h in range(PARTS):
            z_copy(d, h).start()

    for d in order[:-1]:
        leave(d)

    small[2].wait()
    small[3].wait()
    ids = lax.broadcasted_iota(jnp.int32, (-(-Q * group_width // 16) * 16, tok), 0)
    dense = jnp.zeros(ids.shape, F32)
    for k in range(top):
        dense += jnp.where(routes_ref[k:k + 1, :] == ids, probs_ref[k:k + 1, :], 0.0)
    coarse = dense.astype(BF16)
    fine = (dense - coarse.astype(F32)).astype(BF16)
    for d in range(Q):
        pick = picks[d].astype(BF16)
        lines = sum(
            lax.dot_general(part, pick, (((1,), (1,)), ((), ())), preferred_element_type=F32) for part in (coarse, fine))
        base = partner(q, d, Q)[0]
        mine = jnp.zeros((group_width, lanes), F32)
        for g in range(Q):
            mine = jnp.where(base == g, lines[g * group_width:(g + 1) * group_width], mine)
        for i in range(S):
            gate_send[d, i] = mine[i * L:(i + 1) * L]
    gate_recv[0, 0] = gate_send[0, s]
    for d in range(Q):
        loop(1 if d == 0 else 0, S, lambda e: gate_copy(d, e, int(d == 0)).start())
    leave(order[-1])
    away.wait()
    u_copy().start()

    for d in range(Q):
        for k in range(2):
            unpack[d, k] = picks[d][k * RC:(k + 1) * RC].T.astype(BF16)

    row, lane = (lax.broadcasted_iota(jnp.int32, (RC, lanes), i) for i in (0, 1))

    def up_projection(d, k, n):
        base = n * pair
        tokens = jnp.concatenate(
            [gathered[d, k, h, pl.ds(base, pair)].reshape(rows_at_once, W) for h in range(PARTS)], axis=1)
        at_rows = pl.ds(n * rows_at_once, rows_at_once)
        for j in range(L):
            gate = jnp.dot(tokens, w_gate[j], preferred_element_type=F32)
            up = jnp.dot(tokens, w_up[j], preferred_element_type=F32)
            scale = jnp.concatenate([
                jnp.sum(jnp.where(row + k * RC == lane, gate_recv[d, base + b, pl.ds(j, 1), :], 0.0), axis=1, keepdims=True)
                for b in range(pair)
            ], axis=0)
            act = gate / (1.0 + jnp.exp(-gate)) * up
            hidden[d, k, 0, at_rows, j * F:(j + 1) * F] = (act * scale).astype(BF16)

    def down_projection(d, k, n, ready):
        at_rows = pl.ds(n * rows_at_once, rows_at_once)
        part = jnp.dot(hidden[d, k, 0, at_rows], w_down[0].reshape(L * F, H), preferred_element_type=F32)
        ready()
        return part + jnp.dot(hidden[d, k, 1, at_rows], w_down[1].reshape(L * F, H), preferred_element_type=F32)

    def arrived(block, sem):
        remote(block, block, sem, sem, at(me, 1 - c)).wait_recv()

    def sent(block, sem):
        remote(block, block, sem, sem, at(me, 1 - c)).wait_send()

    down_ready, gates_ready, mixed_ready = [], [], []

    def step_a(p, k):
        d = place[p]

        @pl.when(c == k)
        def _():
            for h in range(PARTS):
                z_copy(d, h).wait_recv()
                forward(d, h)

    def step_b(p, k):
        d = place[p]

        def one(e):
            for h in range(PARTS):
                x_copy(d, e, h).wait_recv()
                t_copy(d, e, h).start()
        pl.when(c == k)(lambda: loop(1, S, one))

    def step_g(p, k):
        d = place[p]
        if not gates_ready:
            for copy in weights:
                copy.wait()
        if p not in gates_ready:
            arrived(gate_recv.at[d, pl.ds(1, S - 1)] if p == 0 else gate_recv.at[d], gate_rs.at[d])
            gates_ready.append(p)

        pl.when(c != k)(lambda: arrived(gathered.at[d, 1 - c], t_rs.at[d]))
        if S == pair:
            up_projection(d, k, 0)
        else:
            lax.fori_loop(0, S // pair, lambda n, carry: (up_projection(d, k, n), carry)[1], 0)
        v_copy(d, k).start()

    def step_d(p, k):
        d = place[p]
        if not down_ready:
            u_copy().wait_recv()
            down_ready.append(True)
        out = down_projection(d, k, 0, v_copy(d, k).wait_recv)
        for e in range(1, pair):
            r_send[d, k, e - 1] = out[e * RC:(e + 1) * RC].astype(BF16)
        own_sum[d, k] = out[:RC]
        if S > pair:
            def some(n, carry):
                out = down_projection(d, k, n, lambda: None)
                r_send[d, k, pl.ds(n * pair - 1, pair)] = out.astype(BF16).reshape(pair, RC, H)
                return carry
            lax.fori_loop(1, S // pair, some, 0)
        loop(1, S, lambda e: r_copy(d, e, k).start())

    def step_f(p, k):
        d = place[p]

        arrived(r_recv.at[d, k], r_rs.at[d, k])
        total = own_sum[d, k]
        if S <= 8:
            for e in range(1, S):
                total = total + r_recv[d, k, e - 1].astype(F32)
        else:
            total = lax.fori_loop(1, S, lambda e, total: total + r_recv[d, k, e - 1].astype(F32), total)
        if p == 0:
            home_recv[0, k] = total.astype(BF16)
        else:
            home_send[d - 1, k] = total.astype(BF16)
            h_copy(d, k).start()

    def step_m(p, k):
        d = place[p]
        if p > 0:
            h_copy(d, k).wait_recv()
        term = jnp.dot(unpack[d, k], home_recv[d, k], preferred_element_type=F32)
        mixed[...] = mixed[...] + term if mixed_ready else term
        mixed_ready.append(True)

    actions = {"A": step_a, "B": step_b, "G": step_g, "D": step_d, "F": step_f, "M": step_m}

    steps = STEPS
    if Q != 4:
        units = [f"{p}{k}" for p in range(Q) for k in (1, 0)]
        steps = ["A" + u for u in units[2:]] + [x + u for x in "BGDFM" for u in units]
    for step in steps:
        actions[step[0]](*(int(i) for i in step[1:]))

    total = mixed[...]
    squares = jnp.sum(total * total, axis=1, keepdims=True)
    sq_send[...] = jnp.broadcast_to(squares, sq_send.shape)
    sq_copy = remote(sq_send, sq_recv, q_ss, q_rs, at(me, 1 - c))
    sq_copy.start()
    u_copy().wait_send()
    sent(gate_send.at[pl.ds(1, Q - 1)], gate_ss.at[0])
    sent(gate_send.at[0, pl.ds(1, S - 1)], gate_ss.at[1])
    sent(sendz, z_ss)
    sent(gathered.at[:, c, :, pl.ds(1, S - 1)], x_ss)
    sent(gathered.at[:, c], t_ss)
    sent(hidden.at[:, :, 0], v_ss)
    sent(r_send, r_ss)
    sent(home_send, h_ss)
    sq_copy.wait()
    norm = lax.rsqrt((squares + sq_recv[:, 0:1]) / width + EPS)
    out_ref[...] = (total * norm * out_gain_ref[...]).astype(BF16)


def body(tokens, in_gain, routing, gate_prob, w_gate, w_up, w_down, out_gain):
    N = lax.axis_size("ep")
    L, D, F = w_gate.shape
    tok, top = routing.shape
    H = out_gain.shape[0]
    group_width = L * N // GROUPS
    cap = max(2, tok * top // (2 * group_width))
    R = min(tok, group_width * cap // top)
    R = -(-R // 16) * 16
    Q, S, K = GROUPS, N // GROUPS, 2
    RC = R // K
    lanes = -(-R // 128) * 128
    vmem = pl.BlockSpec(memory_space=pltpu.VMEM)
    hbm = pl.BlockSpec(memory_space=pl.ANY)
    dma = pltpu.SemaphoreType.DMA
    return pl.pallas_call(
        functools.partial(kernel, Q, S, R),
        out_shape=pltpu.VMEM((tok, H), BF16),
        in_specs=[hbm] * 8,
        out_specs=vmem,
        scratch_shapes=[
            pltpu.VMEM((top, tok), jnp.int32),
            pltpu.VMEM((top, tok), F32),
            pltpu.VMEM((1, D), F32),
            pltpu.VMEM((1, H), F32),
            pltpu.VMEM((tok, D), BF16),
            pltpu.VMEM((Q - 1, PARTS, RC, D // PARTS), BF16),
            pltpu.VMEM((Q, K, PARTS, S, RC, D // PARTS), BF16),
            pltpu.VMEM((Q, K, tok, RC), BF16),
            pltpu.VMEM((Q, S, L, lanes), F32),
            pltpu.VMEM((Q, S, L, lanes), F32),
            pltpu.VMEM((L, D, F), BF16),
            pltpu.VMEM((L, D, F), BF16),
            pltpu.VMEM((2, L, F, H), BF16),
            pltpu.VMEM((L, F, H), BF16),
            pltpu.VMEM((Q, K, 2, S * RC, L * F), BF16),
            pltpu.VMEM((Q, K, S - 1, RC, H), BF16),
            pltpu.VMEM((Q, K, RC, H), F32),
            pltpu.VMEM((Q, K, S - 1, RC, H), BF16),
            pltpu.VMEM((Q - 1, K, RC, H), BF16),
            pltpu.VMEM((Q, K, RC, H), BF16),
            pltpu.VMEM((tok, H), F32),
            pltpu.VMEM((tok, 128), F32),
            pltpu.VMEM((tok, 128), F32),
            dma((5,)), dma((4,)), dma((2,)), dma((Q,)), dma, dma((Q - 1, PARTS)), dma, dma((Q, S - 1, PARTS)),
            dma, dma((Q,)), dma, dma, dma, dma((Q, K)), dma, dma((Q, K)), dma, dma((Q - 1, K)), dma, dma,
        ],
        compiler_params=pltpu.CompilerParams(
            collective_id=0, has_side_effects=True, vmem_limit_bytes=64 * 1000 * 1000
        ),
    )(routing.T, gate_prob.T, in_gain.reshape(1, D), out_gain.reshape(1, H), tokens, w_gate, w_up, w_down)


def solution(mesh):
    placed = (
        P(("grp", "ep"), None),
        P(),
        P(("grp", "ep"), None),
        P(("grp", "ep"), None),
        P("ep", None, "tp"),
        P("ep", None, "tp"),
        P("ep", "tp", None),
        P("tp"),
    )
    return jax.shard_map(
        body, mesh=mesh, in_specs=placed, out_specs=P(("grp", "ep"), "tp"), check_vma=False
    )
```

```python
import functools

import jax
import jax.numpy as jnp
from jax import lax
from jax.experimental import pallas as pl
from jax.experimental.pallas import tpu as pltpu
from jax.sharding import PartitionSpec as P

GROUPS = 4
EPS = 1e-06
MESH = pl.DeviceIdType.MESH
F32 = jnp.float32
BF16 = jnp.bfloat16

STEPS = (
    "B01", "A20", "A21", "A30", "B00", "A31", "B21", "G21", "B20", "A11", "B31", "D21",
    "G20", "A10", "B11", "G31", "B30", "D20", "F21", "G11", "D31", "B10", "G30", "D11",
    "F20", "G10", "D30", "G00", "F31", "D10", "F11", "G01", "F30", "D00", "D01", "F10",
    "F00", "M20", "M11", "M31", "M00", "M21", "F01", "M01", "M10", "M30",
)
PLACES = ((2, 3, 1), (3, 2, 1), (3, 2, 1), (2, 3, 1))
ORDERS = ((3, 2, 1), (2, 1, 3), (2, 1, 3), (3, 2, 1))
PARTS = 4


def loop(low, high, step):
    if high - low <= 8:
        for i in range(low, high):
            step(i)
    else:
        lax.fori_loop(low, high, lambda i, carry: (step(i), carry)[1], 0)


def partner(q, d, count):
    if count & (count - 1):
        return lax.rem(q + d, count), lax.rem(q + count - d, count)
    other, bit = 0, 1
    while bit < count:
        mine, theirs = (q // bit) % 2, (d // bit) % 2
        other = other + bit * (mine + theirs - 2 * mine * theirs)
        bit *= 2
    return other, other


def kernel(
    group_count, span, rows,
    routes_hbm, probs_hbm, in_gain_hbm, out_gain_hbm, tokens_hbm, gate_hbm, up_hbm, down_hbm,
    out_ref,
    routes_ref, probs_ref, in_gain_ref, out_gain_ref, tokens_ref, sendz, gathered, unpack, gate_send, gate_recv, w_gate, w_up, w_down, spare, hidden,
    r_send, own_sum, r_recv, home_send, home_recv, mixed, sq_send, sq_recv,
    tok_sem, w_sem, gate_ss, gate_rs, z_ss, z_rs, x_ss, x_rs, t_ss, t_rs, u_ss, u_rs, v_ss, v_rs,
    r_ss, r_rs, h_ss, h_rs, q_ss, q_rs,
):
    Q, S, R = group_count, span, rows
    N = Q * S
    RC = R // 2
    top, tok = routes_ref.shape
    width = tokens_ref.shape[1]
    H = out_ref.shape[1]
    L, _, F = gate_hbm.shape
    W = width // PARTS
    group_width = S * L
    lanes = gate_send.shape[-1]
    me = lax.axis_index("ep")
    c = lax.axis_index("tp")
    q, s = me // S, lax.rem(me, S)
    if Q == 4:
        digit = (1 + 3 * (q % 2)) * (1 + 15 * (q // 2))

        def look_up(table):
            return [sum(row[i] * 4 ** z for z, row in enumerate(table)) // digit % 4 for i in range(3)]
        place, order = [0] + look_up(PLACES), look_up(ORDERS)
    else:
        place, order = list(range(Q)), list(range(1, Q))
    pair = 2 if S % 2 == 0 else 1
    rows_at_once = pair * RC

    def at(ep, tp=None):
        return {"ep": ep, "tp": c if tp is None else tp}

    def remote(src, dst, ss, rs, dev):
        return pltpu.make_async_remote_copy(
            src_ref=src, dst_ref=dst, send_sem=ss, recv_sem=rs, device_id=dev, device_id_type=MESH
        )

    def chunk(k):
        return pl.ds(k * RC, RC)

    small = [
        pltpu.make_async_copy(src, dst, tok_sem.at[i]) for i, (src, dst) in enumerate((
            (routes_hbm, routes_ref), (in_gain_hbm, in_gain_ref), (probs_hbm, probs_ref), (out_gain_hbm, out_gain_ref)))
    ]
    tok_copy = pltpu.make_async_copy(tokens_hbm, tokens_ref, tok_sem.at[4])
    small[0].start()
    tok_copy.start()
    for copy in small[1:]:
        copy.start()

    barrier = pltpu.get_barrier_semaphore()
    loop(1, N, lambda p: pl.semaphore_signal(
        barrier, inc=1, device_id=at(lax.rem(me + p, N)), device_id_type=MESH))
    pl.semaphore_signal(barrier, inc=1, device_id=at(me, 1 - c), device_id_type=MESH)

    own_cols = pl.ds(pl.multiple_of(c * H, H), H)
    other_cols = pl.ds(pl.multiple_of((1 - c) * H, H), H)
    weights = [
        pltpu.make_async_copy(gate_hbm, w_gate, w_sem.at[0]),
        pltpu.make_async_copy(up_hbm, w_up, w_sem.at[1]),
        pltpu.make_async_copy(down_hbm.at[:, :, own_cols], w_down.at[0], w_sem.at[2]),
    ]
    away = pltpu.make_async_copy(down_hbm.at[:, :, other_cols], spare, w_sem.at[3])

    small[0].wait()
    first = routes_ref[0:1, :]
    row_group = lax.broadcasted_iota(jnp.int32, (16, tok), 0)
    groups = jnp.full((16, tok), -1, jnp.int32)
    for d in range(Q):
        groups = jnp.where(row_group == d, partner(q, d, Q)[0], groups)
    member = (groups >= 0) & (first >= groups * group_width) & (first < (groups + 1) * group_width)
    earlier = lax.broadcasted_iota(jnp.int32, (tok, tok), 0) < lax.broadcasted_iota(jnp.int32, (tok, tok), 1)
    rank = jnp.dot(
        jnp.where(member, 1.0, 0.0).astype(BF16), jnp.where(earlier, 1.0, 0.0).astype(BF16),
        preferred_element_type=F32,
    ).astype(jnp.int32)
    slots = lax.broadcasted_iota(jnp.int32, (lanes, tok), 0)
    picks = []
    for d in range(Q):
        low = partner(q, d, Q)[0] * group_width
        inside = (first >= low) & (first < low + group_width)
        picks.append(jnp.where((rank[d:d + 1, :] == slots) & inside, 1.0, 0.0))

    tok_copy.wait()
    small[1].wait()
    for copy in [away] + weights:
        copy.start()
    floats = tokens_ref[...].astype(F32)
    inv = lax.rsqrt(jnp.mean(floats * floats, axis=-1, keepdims=True) + EPS)
    normed = (tokens_ref[...].astype(F32) * inv * in_gain_ref[...]).astype(BF16)
    for d in range(Q):
        pick = jnp.where(c == 0, picks[d][:RC], picks[d][RC:R]).astype(BF16)
        block = jnp.dot(pick, normed, preferred_element_type=F32).astype(BF16)
        for h in range(PARTS):
            if d == 0:
                gathered[0, c, h, 0] = block[:, h * W:(h + 1) * W]
            else:
                sendz[d - 1, h] = block[:, h * W:(h + 1) * W]

    pl.semaphore_wait(barrier, N)

    def z_copy(d, h):
        return remote(
            sendz.at[d - 1, h], gathered.at[d, c, h, 0], z_ss, z_rs.at[d - 1, h], at(partner(q, d, Q)[0] * S + s))

    def x_copy(d, e, h):
        return remote(
            gathered.at[d, c, h, 0], gathered.at[d, c, h, e], x_ss, x_rs.at[d, e - 1, h],
            at(q * S + lax.rem(s + e, S)),
        )

    def t_copy(d, e, h):
        block = gathered.at[d, c, h, e]
        return remote(block, block, t_ss, t_rs.at[d], at(me, 1 - c))

    def gate_copy(d, e, near):
        return remote(
            gate_send.at[d, lax.rem(s + e, S)], gate_recv.at[d, e], gate_ss.at[near], gate_rs.at[d],
            at(partner(q, d, Q)[0] * S + lax.rem(s + e, S)),
        )

    def u_copy():
        return remote(spare, w_down.at[1], u_ss, u_rs, at(me, 1 - c))

    def v_copy(d, k):
        return remote(hidden.at[d, k, 0], hidden.at[d, k, 1], v_ss, v_rs.at[d, k], at(me, 1 - c))

    def r_copy(d, e, k):
        return remote(
            r_send.at[d, k, e - 1], r_recv.at[d, k, e - 1], r_ss, r_rs.at[d, k],
            at(q * S + lax.rem(s + S - e, S)),
        )

    def h_copy(d, k):
        return remote(
            home_send.at[d - 1, k], home_recv.at[d, k], h_ss, h_rs.at[d - 1, k], at(partner(q, d, Q)[1] * S + s))

    def forward(d, h):
        loop(1, S, lambda e: x_copy(d, e, h).start())
        t_copy(d, 0, h).start()

    for h in range(PARTS):
        forward(0, h)
    def leave(d):
        for h in range(PARTS):
            z_copy(d, h).start()

    for d in order[:-1]:
        leave(d)

    small[2].wait()
    small[3].wait()
    ids = lax.broadcasted_iota(jnp.int32, (-(-Q * group_width // 16) * 16, tok), 0)
    dense = jnp.zeros(ids.shape, F32)
    for k in range(top):
        dense += jnp.where(routes_ref[k:k + 1, :] == ids, probs_ref[k:k + 1, :], 0.0)
    coarse = dense.astype(BF16)
    fine = (dense - coarse.astype(F32)).astype(BF16)
    for d in range(Q):
        pick = picks[d].astype(BF16)
        lines = sum(
            lax.dot_general(part, pick, (((1,), (1,)), ((), ())), preferred_element_type=F32) for part in (coarse, fine))
        base = partner(q, d, Q)[0]
        mine = jnp.zeros((group_width, lanes), F32)
        for g in range(Q):
            mine = jnp.where(base == g, lines[g * group_width:(g + 1) * group_width], mine)
        for i in range(S):
            gate_send[d, i] = mine[i * L:(i + 1) * L]
    gate_recv[0, 0] = gate_send[0, s]
    for d in range(Q):
        loop(1 if d == 0 else 0, S, lambda e: gate_copy(d, e, int(d == 0)).start())
    leave(order[-1])
    away.wait()
    u_copy().start()

    for d in range(Q):
        for k in range(2):
            unpack[d, k] = picks[d][k * RC:(k + 1) * RC].T.astype(BF16)

    row, lane = (lax.broadcasted_iota(jnp.int32, (RC, lanes), i) for i in (0, 1))

    def up_projection(d, k, n):
        base = n * pair
        tokens = jnp.concatenate(
            [gathered[d, k, h, pl.ds(base, pair)].reshape(rows_at_once, W) for h in range(PARTS)], axis=1)
        at_rows = pl.ds(n * rows_at_once, rows_at_once)
        for j in range(L):
            gate = jnp.dot(tokens, w_gate[j], preferred_element_type=F32)
            up = jnp.dot(tokens, w_up[j], preferred_element_type=F32)
            scale = jnp.concatenate([
                jnp.sum(jnp.where(row + k * RC == lane, gate_recv[d, base + b, pl.ds(j, 1), :], 0.0), axis=1, keepdims=True)
                for b in range(pair)
            ], axis=0)
            act = gate / (1.0 + jnp.exp(-gate)) * up
            hidden[d, k, 0, at_rows, j * F:(j + 1) * F] = (act * scale).astype(BF16)

    def down_projection(d, k, n, ready):
        at_rows = pl.ds(n * rows_at_once, rows_at_once)
        part = jnp.dot(hidden[d, k, 0, at_rows], w_down[0].reshape(L * F, H), preferred_element_type=F32)
        ready()
        return part + jnp.dot(hidden[d, k, 1, at_rows], w_down[1].reshape(L * F, H), preferred_element_type=F32)

    def arrived(block, sem):
        remote(block, block, sem, sem, at(me, 1 - c)).wait_recv()

    def sent(block, sem):
        remote(block, block, sem, sem, at(me, 1 - c)).wait_send()

    down_ready, gates_ready, mixed_ready = [], [], []

    def step_a(p, k):
        d = place[p]

        @pl.when(c == k)
        def _():
            for h in range(PARTS):
                z_copy(d, h).wait_recv()
                forward(d, h)

    def step_b(p, k):
        d = place[p]

        def one(e):
            for h in range(PARTS):
                x_copy(d, e, h).wait_recv()
                t_copy(d, e, h).start()
        pl.when(c == k)(lambda: loop(1, S, one))

    def step_g(p, k):
        d = place[p]
        if not gates_ready:
            for copy in weights:
                copy.wait()
        if p not in gates_ready:
            arrived(gate_recv.at[d, pl.ds(1, S - 1)] if p == 0 else gate_recv.at[d], gate_rs.at[d])
            gates_ready.append(p)

        pl.when(c != k)(lambda: arrived(gathered.at[d, 1 - c], t_rs.at[d]))
        if S == pair:
            up_projection(d, k, 0)
        else:
            lax.fori_loop(0, S // pair, lambda n, carry: (up_projection(d, k, n), carry)[1], 0)
        v_copy(d, k).start()

    def step_d(p, k):
        d = place[p]
        if not down_ready:
            u_copy().wait_recv()
            down_ready.append(True)
        out = down_projection(d, k, 0, v_copy(d, k).wait_recv)
        for e in range(1, pair):
            r_send[d, k, e - 1] = out[e * RC:(e + 1) * RC].astype(BF16)
        own_sum[d, k] = out[:RC]
        if S > pair:
            def some(n, carry):
                out = down_projection(d, k, n, lambda: None)
                r_send[d, k, pl.ds(n * pair - 1, pair)] = out.astype(BF16).reshape(pair, RC, H)
                return carry
            lax.fori_loop(1, S // pair, some, 0)
        loop(1, S, lambda e: r_copy(d, e, k).start())

    def step_f(p, k):
        d = place[p]

        arrived(r_recv.at[d, k], r_rs.at[d, k])
        total = own_sum[d, k]
        if S <= 8:
            for e in range(1, S):
                total = total + r_recv[d, k, e - 1].astype(F32)
        else:
            total = lax.fori_loop(1, S, lambda e, total: total + r_recv[d, k, e - 1].astype(F32), total)
        if p == 0:
            home_recv[0, k] = total.astype(BF16)
        else:
            home_send[d - 1, k] = total.astype(BF16)
            h_copy(d, k).start()

    def step_m(p, k):
        d = place[p]
        if p > 0:
            h_copy(d, k).wait_recv()
        term = jnp.dot(unpack[d, k], home_recv[d, k], preferred_element_type=F32)
        mixed[...] = mixed[...] + term if mixed_ready else term
        mixed_ready.append(True)

    actions = {"A": step_a, "B": step_b, "G": step_g, "D": step_d, "F": step_f, "M": step_m}

    steps = STEPS
    if Q != 4:
        units = [f"{p}{k}" for p in range(Q) for k in (1, 0)]
        steps = ["A" + u for u in units[2:]] + [x + u for x in "BGDFM" for u in units]
    for step in steps:
        actions[step[0]](*(int(i) for i in step[1:]))

    total = mixed[...]
    squares = jnp.sum(total * total, axis=1, keepdims=True)
    sq_send[...] = jnp.broadcast_to(squares, sq_send.shape)
    sq_copy = remote(sq_send, sq_recv, q_ss, q_rs, at(me, 1 - c))
    sq_copy.start()
    u_copy().wait_send()
    sent(gate_send.at[pl.ds(1, Q - 1)], gate_ss.at[0])
    sent(gate_send.at[0, pl.ds(1, S - 1)], gate_ss.at[1])
    sent(sendz, z_ss)
    sent(gathered.at[:, c, :, pl.ds(1, S - 1)], x_ss)
    sent(gathered.at[:, c], t_ss)
    sent(hidden.at[:, :, 0], v_ss)
    sent(r_send, r_ss)
    sent(home_send, h_ss)
    sq_copy.wait()
    norm = lax.rsqrt((squares + sq_recv[:, 0:1]) / width + EPS)
    out_ref[...] = (total * norm * out_gain_ref[...]).astype(BF16)


def body(tokens, in_gain, routing, gate_prob, w_gate, w_up, w_down, out_gain):
    N = lax.axis_size("ep")
    L, D, F = w_gate.shape
    tok, top = routing.shape
    H = out_gain.shape[0]
    group_width = L * N // GROUPS
    cap = max(2, tok * top // (2 * group_width))
    R = min(tok, group_width * cap // top)
    R = -(-R // 16) * 16
    Q, S, K = GROUPS, N // GROUPS, 2
    RC = R // K
    lanes = -(-R // 128) * 128
    vmem = pl.BlockSpec(memory_space=pltpu.VMEM)
    hbm = pl.BlockSpec(memory_space=pl.ANY)
    dma = pltpu.SemaphoreType.DMA
    return pl.pallas_call(
        functools.partial(kernel, Q, S, R),
        out_shape=pltpu.VMEM((tok, H), BF16),
        in_specs=[hbm] * 8,
        out_specs=vmem,
        scratch_shapes=[
            pltpu.VMEM((top, tok), jnp.int32),
            pltpu.VMEM((top, tok), F32),
            pltpu.VMEM((1, D), F32),
            pltpu.VMEM((1, H), F32),
            pltpu.VMEM((tok, D), BF16),
            pltpu.VMEM((Q - 1, PARTS, RC, D // PARTS), BF16),
            pltpu.VMEM((Q, K, PARTS, S, RC, D // PARTS), BF16),
            pltpu.VMEM((Q, K, tok, RC), BF16),
            pltpu.VMEM((Q, S, L, lanes), F32),
            pltpu.VMEM((Q, S, L, lanes), F32),
            pltpu.VMEM((L, D, F), BF16),
            pltpu.VMEM((L, D, F), BF16),
            pltpu.VMEM((2, L, F, H), BF16),
            pltpu.VMEM((L, F, H), BF16),
            pltpu.VMEM((Q, K, 2, S * RC, L * F), BF16),
            pltpu.VMEM((Q, K, S - 1, RC, H), BF16),
            pltpu.VMEM((Q, K, RC, H), F32),
            pltpu.VMEM((Q, K, S - 1, RC, H), BF16),
            pltpu.VMEM((Q - 1, K, RC, H), BF16),
            pltpu.VMEM((Q, K, RC, H), BF16),
            pltpu.VMEM((tok, H), F32),
            pltpu.VMEM((tok, 128), F32),
            pltpu.VMEM((tok, 128), F32),
            dma((5,)), dma((4,)), dma((2,)), dma((Q,)), dma, dma((Q - 1, PARTS)), dma, dma((Q, S - 1, PARTS)),
            dma, dma((Q,)), dma, dma, dma, dma((Q, K)), dma, dma((Q, K)), dma, dma((Q - 1, K)), dma, dma,
        ],
        compiler_params=pltpu.CompilerParams(
            collective_id=0, has_side_effects=True, vmem_limit_bytes=64 * 1000 * 1000
        ),
    )(routing.T, gate_prob.T, in_gain.reshape(1, D), out_gain.reshape(1, H), tokens, w_gate, w_up, w_down)


def solution(mesh):
    placed = (
        P(("grp", "ep"), None),
        P(),
        P(("grp", "ep"), None),
        P(("grp", "ep"), None),
        P("ep", None, "tp"),
        P("ep", None, "tp"),
        P("ep", "tp", None),
        P("tp"),
    )
    return jax.shard_map(
        body, mesh=mesh, in_specs=placed, out_specs=P(("grp", "ep"), "tp"), check_vma=False
    )
```

```python
import functools

import jax
import jax.numpy as jnp
from jax import lax
from jax.experimental import pallas as pl
from jax.experimental.pallas import tpu as pltpu
from jax.sharding import PartitionSpec as P

GROUPS = 4
EPS = 1e-06
MESH = pl.DeviceIdType.MESH
F32 = jnp.float32
BF16 = jnp.bfloat16

STEPS = (
    "B01", "A20", "A21", "A30", "B00", "A31", "B21", "G21", "B20", "A11", "B31", "D21",
    "G20", "A10", "B11", "G31", "B30", "D20", "F21", "G11", "D31", "B10", "G30", "D11",
    "F20", "G10", "D30", "G00", "F31", "D10", "F11", "G01", "F30", "D00", "D01", "F10",
    "F00", "F01", "M20", "M11", "M31", "M00", "M21", "M01", "M10", "M30",
)
PLACES = ((2, 3, 1), (3, 2, 1), (3, 2, 1), (2, 3, 1))
ORDERS = ((3, 2, 1), (2, 1, 3), (2, 1, 3), (3, 2, 1))
PARTS = 4


def loop(low, high, step):
    if high - low <= 8:
        for i in range(low, high):
            step(i)
    else:
        lax.fori_loop(low, high, lambda i, carry: (step(i), carry)[1], 0)


def partner(q, d, count):
    if count & (count - 1):
        return lax.rem(q + d, count), lax.rem(q + count - d, count)
    other, bit = 0, 1
    while bit < count:
        mine, theirs = (q // bit) % 2, (d // bit) % 2
        other = other + bit * (mine + theirs - 2 * mine * theirs)
        bit *= 2
    return other, other


def kernel(
    group_count, span, rows,
    routes_hbm, probs_hbm, in_gain_hbm, out_gain_hbm, tokens_hbm, gate_hbm, up_hbm, down_hbm,
    out_ref,
    routes_ref, probs_ref, in_gain_ref, out_gain_ref, tokens_ref, sendz, gathered, unpack, gate_send, gate_recv, w_gate, w_up, w_down, spare, hidden,
    r_send, own_sum, r_recv, home_send, home_recv, mixed, sq_send, sq_recv,
    tok_sem, w_sem, gate_ss, gate_rs, z_ss, z_rs, x_ss, x_rs, t_ss, t_rs, u_ss, u_rs, v_ss, v_rs,
    r_ss, r_rs, h_ss, h_rs, q_ss, q_rs,
):
    Q, S, R = group_count, span, rows
    N = Q * S
    RC = R // 2
    top, tok = routes_ref.shape
    width = tokens_ref.shape[1]
    H = out_ref.shape[1]
    L, _, F = gate_hbm.shape
    W = width // PARTS
    group_width = S * L
    lanes = gate_send.shape[-1]
    me = lax.axis_index("ep")
    c = lax.axis_index("tp")
    q, s = me // S, lax.rem(me, S)
    if Q == 4:
        digit = (1 + 3 * (q % 2)) * (1 + 15 * (q // 2))

        def look_up(table):
            return [sum(row[i] * 4 ** z for z, row in enumerate(table)) // digit % 4 for i in range(3)]
        place, order = [0] + look_up(PLACES), look_up(ORDERS)
    else:
        place, order = list(range(Q)), list(range(1, Q))
    pair = 2 if S % 2 == 0 else 1
    rows_at_once = pair * RC

    def at(ep, tp=None):
        return {"ep": ep, "tp": c if tp is None else tp}

    def remote(src, dst, ss, rs, dev):
        return pltpu.make_async_remote_copy(
            src_ref=src, dst_ref=dst, send_sem=ss, recv_sem=rs, device_id=dev, device_id_type=MESH
        )

    def chunk(k):
        return pl.ds(k * RC, RC)

    small = [
        pltpu.make_async_copy(src, dst, tok_sem.at[i]) for i, (src, dst) in enumerate((
            (routes_hbm, routes_ref), (in_gain_hbm, in_gain_ref), (probs_hbm, probs_ref), (out_gain_hbm, out_gain_ref)))
    ]
    tok_copy = pltpu.make_async_copy(tokens_hbm, tokens_ref, tok_sem.at[4])
    tok_copy.start()
    small[0].start()

    barrier = pltpu.get_barrier_semaphore()
    for d in reversed(range(Q)):
        loop(1 if d == 0 else 0, S, lambda e: pl.semaphore_signal(
            barrier, inc=1, device_id=at(partner(q, d, Q)[0] * S + lax.rem(s + e, S)), device_id_type=MESH))
    pl.semaphore_signal(barrier, inc=1, device_id=at(me, 1 - c), device_id_type=MESH)
    for copy in small[1:]:
        copy.start()

    own_cols = pl.ds(pl.multiple_of(c * H, H), H)
    other_cols = pl.ds(pl.multiple_of((1 - c) * H, H), H)
    weights = [
        pltpu.make_async_copy(gate_hbm, w_gate, w_sem.at[0]),
        pltpu.make_async_copy(up_hbm, w_up, w_sem.at[1]),
        pltpu.make_async_copy(down_hbm.at[:, :, own_cols], w_down.at[0], w_sem.at[2]),
    ]
    away = pltpu.make_async_copy(down_hbm.at[:, :, other_cols], spare, w_sem.at[3])

    small[0].wait()
    first = routes_ref[0:1, :]
    row_group = lax.broadcasted_iota(jnp.int32, (16, tok), 0)
    groups = jnp.full((16, tok), -1, jnp.int32)
    for d in range(Q):
        groups = jnp.where(row_group == d, partner(q, d, Q)[0], groups)
    member = (groups >= 0) & (first >= groups * group_width) & (first < (groups + 1) * group_width)
    earlier = lax.broadcasted_iota(jnp.int32, (tok, tok), 0) < lax.broadcasted_iota(jnp.int32, (tok, tok), 1)
    rank = jnp.dot(
        jnp.where(member, 1.0, 0.0).astype(BF16), jnp.where(earlier, 1.0, 0.0).astype(BF16),
        preferred_element_type=F32,
    ).astype(jnp.int32)
    slots = lax.broadcasted_iota(jnp.int32, (lanes, tok), 0)
    picks = []
    for d in range(Q):
        low = partner(q, d, Q)[0] * group_width
        inside = (first >= low) & (first < low + group_width)
        picks.append(jnp.where((rank[d:d + 1, :] == slots) & inside, 1.0, 0.0))

    tok_copy.wait()
    small[1].wait()
    for copy in [away] + weights:
        copy.start()
    floats = tokens_ref[...].astype(F32)
    inv = lax.rsqrt(jnp.mean(floats * floats, axis=-1, keepdims=True) + EPS)
    normed = (tokens_ref[...].astype(F32) * inv * in_gain_ref[...]).astype(BF16)
    for d in range(Q):
        pick = jnp.where(c == 0, picks[d][:RC], picks[d][RC:R]).astype(BF16)
        block = jnp.dot(pick, normed, preferred_element_type=F32).astype(BF16)
        for h in range(PARTS):
            if d == 0:
                gathered[0, c, h, 0] = block[:, h * W:(h + 1) * W]
            else:
                sendz[d - 1, h] = block[:, h * W:(h + 1) * W]

    pl.semaphore_wait(barrier, N)

    def z_copy(d, h):
        return remote(
            sendz.at[d - 1, h], gathered.at[d, c, h, 0], z_ss, z_rs.at[d - 1, h], at(partner(q, d, Q)[0] * S + s))

    def x_copy(d, e, h):
        return remote(
            gathered.at[d, c, h, 0], gathered.at[d, c, h, e], x_ss, x_rs.at[d, e - 1, h],
            at(q * S + lax.rem(s + e, S)),
        )

    def t_copy(d, e, h):
        block = gathered.at[d, c, h, e]
        return remote(block, block, t_ss, t_rs.at[d], at(me, 1 - c))

    def gate_copy(d, e, near):
        return remote(
            gate_send.at[d, lax.rem(s + e, S)], gate_recv.at[d, e], gate_ss.at[near], gate_rs.at[d],
            at(partner(q, d, Q)[0] * S + lax.rem(s + e, S)),
        )

    def u_copy():
        return remote(spare, w_down.at[1], u_ss, u_rs, at(me, 1 - c))

    def v_copy(d, k):
        return remote(hidden.at[d, k, 0], hidden.at[d, k, 1], v_ss, v_rs.at[d, k], at(me, 1 - c))

    def r_copy(d, e, k):
        return remote(
            r_send.at[d, k, e - 1], r_recv.at[d, k, e - 1], r_ss, r_rs.at[d, k],
            at(q * S + lax.rem(s + S - e, S)),
        )

    def h_copy(d, k):
        return remote(
            home_send.at[d - 1, k], home_recv.at[d, k], h_ss, h_rs.at[d - 1, k], at(partner(q, d, Q)[1] * S + s))

    def forward(d, h):
        loop(1, S, lambda e: x_copy(d, e, h).start())
        t_copy(d, 0, h).start()

    for h in range(PARTS):
        forward(0, h)
    def q_copy(d, k, p):
        home = at(me, 1 - c) if p == 0 else at(partner(q, d, Q)[1] * S + s, 1 - c)
        return remote(sq_send.at[d, k], sq_recv.at[d, k], q_ss, q_rs.at[d, k], home)

    def leave(d):
        for h in range(PARTS):
            z_copy(d, h).start()

    for d in order[:-1]:
        leave(d)

    small[2].wait()
    small[3].wait()
    ids = lax.broadcasted_iota(jnp.int32, (-(-Q * group_width // 16) * 16, tok), 0)
    dense = jnp.zeros(ids.shape, F32)
    for k in range(top):
        dense += jnp.where(routes_ref[k:k + 1, :] == ids, probs_ref[k:k + 1, :], 0.0)
    coarse = dense.astype(BF16)
    fine = (dense - coarse.astype(F32)).astype(BF16)
    for d in range(Q):
        pick = picks[d].astype(BF16)
        lines = sum(
            lax.dot_general(part, pick, (((1,), (1,)), ((), ())), preferred_element_type=F32) for part in (coarse, fine))
        base = partner(q, d, Q)[0]
        mine = jnp.zeros((group_width, lanes), F32)
        for g in range(Q):
            mine = jnp.where(base == g, lines[g * group_width:(g + 1) * group_width], mine)
        for i in range(S):
            gate_send[d, i] = mine[i * L:(i + 1) * L]
    gate_recv[0, 0] = gate_send[0, s]
    for d in range(Q):
        loop(1 if d == 0 else 0, S, lambda e: gate_copy(d, e, int(d == 0)).start())
    leave(order[-1])
    away.wait()
    u_copy().start()

    for d in range(Q):
        for k in range(2):
            unpack[d, k] = picks[d][k * RC:(k + 1) * RC].T.astype(BF16)

    row, lane = (lax.broadcasted_iota(jnp.int32, (RC, lanes), i) for i in (0, 1))

    def up_projection(d, k, n):
        base = n * pair
        tokens = jnp.concatenate(
            [gathered[d, k, h, pl.ds(base, pair)].reshape(rows_at_once, W) for h in range(PARTS)], axis=1)
        at_rows = pl.ds(n * rows_at_once, rows_at_once)
        for j in range(L):
            gate = jnp.dot(tokens, w_gate[j], preferred_element_type=F32)
            up = jnp.dot(tokens, w_up[j], preferred_element_type=F32)
            scale = jnp.concatenate([
                jnp.sum(jnp.where(row + k * RC == lane, gate_recv[d, base + b, pl.ds(j, 1), :], 0.0), axis=1, keepdims=True)
                for b in range(pair)
            ], axis=0)
            act = gate / (1.0 + jnp.exp(-gate)) * up
            hidden[d, k, 0, at_rows, j * F:(j + 1) * F] = (act * scale).astype(BF16)

    def down_projection(d, k, n, ready):
        at_rows = pl.ds(n * rows_at_once, rows_at_once)
        part = jnp.dot(hidden[d, k, 0, at_rows], w_down[0].reshape(L * F, H), preferred_element_type=F32)
        ready()
        return part + jnp.dot(hidden[d, k, 1, at_rows], w_down[1].reshape(L * F, H), preferred_element_type=F32)

    def arrived(block, sem):
        remote(block, block, sem, sem, at(me, 1 - c)).wait_recv()

    def sent(block, sem):
        remote(block, block, sem, sem, at(me, 1 - c)).wait_send()

    ups_left = [(p, k) for p in range(Q) for k in range(2)]
    down_ready, gates_ready, mixed_ready, unsent = [], [], [], []

    def send_squares():
        units = list(unsent)
        unsent.clear()
        for p, k in units:
            d = place[p]
            rows = (home_recv[0, k] if p == 0 else home_send[d - 1, k]).astype(F32)
            squares = rows * rows
            squares = sum(squares[:, i:i + 128] for i in range(128, H, 128)) + squares[:, :128]
            line = lax.dot_general(
                jnp.ones((8, 128), F32), squares, (((1,), (1,)), ((), ())),
                precision=lax.Precision.HIGHEST, preferred_element_type=F32)
            sq_send[d, k, :, :RC] = line[:1]
        for p, k in units:
            q_copy(place[p], k, p).start()

    def step_a(p, k):
        d = place[p]

        @pl.when(c == k)
        def _():
            for h in range(PARTS):
                z_copy(d, h).wait_recv()
                forward(d, h)

    def step_b(p, k):
        d = place[p]

        def one(e):
            for h in range(PARTS):
                x_copy(d, e, h).wait_recv()
                t_copy(d, e, h).start()
        pl.when(c == k)(lambda: loop(1, S, one))

    def step_g(p, k):
        d = place[p]
        ups_left.remove((p, k))
        if not gates_ready:
            for copy in weights:
                copy.wait()
        if p not in gates_ready:
            arrived(gate_recv.at[d, pl.ds(1, S - 1)] if p == 0 else gate_recv.at[d], gate_rs.at[d])
            gates_ready.append(p)

        pl.when(c != k)(lambda: arrived(gathered.at[d, 1 - c], t_rs.at[d]))
        if S == pair:
            up_projection(d, k, 0)
        else:
            lax.fori_loop(0, S // pair, lambda n, carry: (up_projection(d, k, n), carry)[1], 0)
        v_copy(d, k).start()
        send_squares()

    def step_d(p, k):
        d = place[p]
        if not down_ready:
            u_copy().wait_recv()
            down_ready.append(True)
        out = down_projection(d, k, 0, v_copy(d, k).wait_recv)
        for e in range(1, pair):
            r_send[d, k, e - 1] = out[e * RC:(e + 1) * RC].astype(BF16)
        own_sum[d, k] = out[:RC]
        if S > pair:
            def some(n, carry):
                out = down_projection(d, k, n, lambda: None)
                r_send[d, k, pl.ds(n * pair - 1, pair)] = out.astype(BF16).reshape(pair, RC, H)
                return carry
            lax.fori_loop(1, S // pair, some, 0)
        loop(1, S, lambda e: r_copy(d, e, k).start())

    def step_f(p, k):
        d = place[p]

        arrived(r_recv.at[d, k], r_rs.at[d, k])
        total = own_sum[d, k]
        if S <= 8:
            for e in range(1, S):
                total = total + r_recv[d, k, e - 1].astype(F32)
        else:
            total = lax.fori_loop(1, S, lambda e, total: total + r_recv[d, k, e - 1].astype(F32), total)
        if p == 0:
            home_recv[0, k] = total.astype(BF16)
        else:
            home_send[d - 1, k] = total.astype(BF16)
            h_copy(d, k).start()
        unsent.append((p, k))
        if not ups_left:
            send_squares()

    def step_m(p, k):
        d = place[p]
        if p > 0:
            h_copy(d, k).wait_recv()
        term = jnp.dot(unpack[d, k], home_recv[d, k], preferred_element_type=F32)
        mixed[...] = mixed[...] + term if mixed_ready else term
        mixed_ready.append(True)

    actions = {"A": step_a, "B": step_b, "G": step_g, "D": step_d, "F": step_f, "M": step_m}

    steps = STEPS
    if Q != 4:
        units = [f"{p}{k}" for p in range(Q) for k in (1, 0)]
        steps = ["A" + u for u in units[2:]] + [x + u for x in "BGDFM" for u in units]
    for step in steps:
        actions[step[0]](*(int(i) for i in step[1:]))

    total = mixed[...]
    squares = jnp.sum(total * total, axis=1, keepdims=True)
    u_copy().wait_send()
    sent(gate_send.at[pl.ds(1, Q - 1)], gate_ss.at[0])
    sent(gate_send.at[0, pl.ds(1, S - 1)], gate_ss.at[1])
    sent(sendz, z_ss)
    sent(gathered.at[:, c, :, pl.ds(1, S - 1)], x_ss)
    sent(gathered.at[:, c], t_ss)
    sent(hidden.at[:, :, 0], v_ss)
    sent(r_send, r_ss)
    sent(home_send, h_ss)
    sent(sq_send, q_ss)
    theirs = jnp.zeros((tok, RC), F32)
    for p in range(Q):
        for k in range(2):
            q_copy(place[p], k, p).wait_recv()
            theirs += unpack[place[p], k].astype(F32) * sq_recv[place[p], k, :, :RC]
    squares = squares + jnp.sum(theirs, axis=1, keepdims=True)
    out_ref[...] = (total * lax.rsqrt(squares / width + EPS) * out_gain_ref[...]).astype(BF16)


def body(tokens, in_gain, routing, gate_prob, w_gate, w_up, w_down, out_gain):
    N = lax.axis_size("ep")
    L, D, F = w_gate.shape
    tok, top = routing.shape
    H = out_gain.shape[0]
    group_width = L * N // GROUPS
    cap = max(2, tok * top // (2 * group_width))
    R = min(tok, group_width * cap // top)
    R = -(-R // 16) * 16
    Q, S, K = GROUPS, N // GROUPS, 2
    RC = R // K
    lanes = -(-R // 128) * 128
    vmem = pl.BlockSpec(memory_space=pltpu.VMEM)
    hbm = pl.BlockSpec(memory_space=pl.ANY)
    dma = pltpu.SemaphoreType.DMA
    return pl.pallas_call(
        functools.partial(kernel, Q, S, R),
        out_shape=pltpu.VMEM((tok, H), BF16),
        in_specs=[hbm] * 8,
        out_specs=vmem,
        scratch_shapes=[
            pltpu.VMEM((top, tok), jnp.int32),
            pltpu.VMEM((top, tok), F32),
            pltpu.VMEM((1, D), F32),
            pltpu.VMEM((1, H), F32),
            pltpu.VMEM((tok, D), BF16),
            pltpu.VMEM((Q - 1, PARTS, RC, D // PARTS), BF16),
            pltpu.VMEM((Q, K, PARTS, S, RC, D // PARTS), BF16),
            pltpu.VMEM((Q, K, tok, RC), BF16),
            pltpu.VMEM((Q, S, L, lanes), F32),
            pltpu.VMEM((Q, S, L, lanes), F32),
            pltpu.VMEM((L, D, F), BF16),
            pltpu.VMEM((L, D, F), BF16),
            pltpu.VMEM((2, L, F, H), BF16),
            pltpu.VMEM((L, F, H), BF16),
            pltpu.VMEM((Q, K, 2, S * RC, L * F), BF16),
            pltpu.VMEM((Q, K, S - 1, RC, H), BF16),
            pltpu.VMEM((Q, K, RC, H), F32),
            pltpu.VMEM((Q, K, S - 1, RC, H), BF16),
            pltpu.VMEM((Q - 1, K, RC, H), BF16),
            pltpu.VMEM((Q, K, RC, H), BF16),
            pltpu.VMEM((tok, H), F32),
            pltpu.VMEM((Q, K, 1, lanes), F32),
            pltpu.VMEM((Q, K, 1, lanes), F32),
            dma((5,)), dma((4,)), dma((2,)), dma((Q,)), dma, dma((Q - 1, PARTS)), dma, dma((Q, S - 1, PARTS)),
            dma, dma((Q,)), dma, dma, dma, dma((Q, K)), dma, dma((Q, K)), dma, dma((Q - 1, K)), dma, dma((Q, K)),
        ],
        compiler_params=pltpu.CompilerParams(
            collective_id=0, has_side_effects=True, vmem_limit_bytes=64 * 1000 * 1000
        ),
    )(routing.T, gate_prob.T, in_gain.reshape(1, D), out_gain.reshape(1, H), tokens, w_gate, w_up, w_down)


def solution(mesh):
    placed = (
        P(("grp", "ep"), None),
        P(),
        P(("grp", "ep"), None),
        P(("grp", "ep"), None),
        P("ep", None, "tp"),
        P("ep", None, "tp"),
        P("ep", "tp", None),
        P("tp"),
    )
    return jax.shard_map(
        body, mesh=mesh, in_specs=placed, out_specs=P(("grp", "ep"), "tp"), check_vma=False
    )
```

```python
import functools

import jax
import jax.numpy as jnp
from jax import lax
from jax.experimental import pallas as pl
from jax.experimental.pallas import tpu as pltpu
from jax.sharding import PartitionSpec as P

GROUPS = 4
EPS = 1e-06
MESH = pl.DeviceIdType.MESH
F32 = jnp.float32
BF16 = jnp.bfloat16

STEPS = (
    "A20", "B00", "A21", "A30", "A31", "B21", "G21", "B20", "A11", "B31", "D21", "G20",
    "A10", "B11", "G31", "B30", "D20", "G11", "F21", "D31", "G30", "B10", "B01", "D11",
    "D30", "F20", "G10", "F31", "G00", "D10", "F11", "G01", "F30", "D00", "D01", "F10",
    "M31", "M20", "F00", "F01", "M11", "M00", "M21", "M01", "M30", "M10",
)
PLACES = ((2, 3, 1), (3, 2, 1), (3, 2, 1), (2, 3, 1))
ORDERS = ((3, 2, 1), (1, 2, 3), (1, 2, 3), (3, 2, 1))
PARTS = 4


def loop(low, high, step):
    if high - low <= 8:
        for i in range(low, high):
            step(i)
    else:
        lax.fori_loop(low, high, lambda i, carry: (step(i), carry)[1], 0)


def partner(q, d, count):
    if count & (count - 1):
        return lax.rem(q + d, count), lax.rem(q + count - d, count)
    other, bit = 0, 1
    while bit < count:
        mine, theirs = (q // bit) % 2, (d // bit) % 2
        other = other + bit * (mine + theirs - 2 * mine * theirs)
        bit *= 2
    return other, other


def kernel(
    group_count, span, rows,
    routes_hbm, probs_hbm, in_gain_hbm, out_gain_hbm, tokens_hbm, gate_hbm, up_hbm, down_hbm,
    out_ref,
    routes_ref, probs_ref, in_gain_ref, out_gain_ref, tokens_ref, sendz, gathered, unpack, gate_send, gate_recv, w_gate, w_up, w_down, spare, hidden,
    r_send, own_sum, r_recv, home_send, home_recv, mixed, sq_send, sq_recv,
    tok_sem, w_sem, gate_ss, gate_rs, z_ss, z_rs, x_ss, x_rs, t_ss, t_rs, u_ss, u_rs, v_ss, v_rs,
    r_ss, r_rs, h_ss, h_rs, q_ss, q_rs,
):
    Q, S, R = group_count, span, rows
    N = Q * S
    RC = R // 2
    top, tok = routes_ref.shape
    width = tokens_ref.shape[1]
    H = out_ref.shape[1]
    L, _, F = gate_hbm.shape
    W = width // PARTS
    group_width = S * L
    lanes = gate_send.shape[-1]
    me = lax.axis_index("ep")
    c = lax.axis_index("tp")
    q, s = me // S, lax.rem(me, S)
    if Q == 4:
        digit = (1 + 3 * (q % 2)) * (1 + 15 * (q // 2))

        def look_up(table):
            return [sum(row[i] * 4 ** z for z, row in enumerate(table)) // digit % 4 for i in range(3)]
        place, order = [0] + look_up(PLACES), look_up(ORDERS)
    else:
        place, order = list(range(Q)), list(range(1, Q))
    pair = 2 if S % 2 == 0 else 1
    rows_at_once = pair * RC

    def at(ep, tp=None):
        return {"ep": ep, "tp": c if tp is None else tp}

    def remote(src, dst, ss, rs, dev):
        return pltpu.make_async_remote_copy(
            src_ref=src, dst_ref=dst, send_sem=ss, recv_sem=rs, device_id=dev, device_id_type=MESH
        )

    def chunk(k):
        return pl.ds(k * RC, RC)

    small = [
        pltpu.make_async_copy(src, dst, tok_sem.at[i]) for i, (src, dst) in enumerate((
            (routes_hbm, routes_ref), (in_gain_hbm, in_gain_ref), (probs_hbm, probs_ref), (out_gain_hbm, out_gain_ref)))
    ]
    tok_copy = pltpu.make_async_copy(tokens_hbm, tokens_ref, tok_sem.at[4])
    tok_copy.start()
    small[0].start()

    barrier = pltpu.get_barrier_semaphore()
    for d in reversed(range(Q)):
        loop(1 if d == 0 else 0, S, lambda e: pl.semaphore_signal(
            barrier, inc=1, device_id=at(partner(q, d, Q)[0] * S + lax.rem(s + e, S)), device_id_type=MESH))
    pl.semaphore_signal(barrier, inc=1, device_id=at(me, 1 - c), device_id_type=MESH)
    for copy in small[1:]:
        copy.start()

    own_cols = pl.ds(pl.multiple_of(c * H, H), H)
    other_cols = pl.ds(pl.multiple_of((1 - c) * H, H), H)
    weights = [
        pltpu.make_async_copy(gate_hbm, w_gate, w_sem.at[0]),
        pltpu.make_async_copy(up_hbm, w_up, w_sem.at[1]),
        pltpu.make_async_copy(down_hbm.at[:, :, own_cols], w_down.at[0], w_sem.at[2]),
    ]
    away = pltpu.make_async_copy(down_hbm.at[:, :, other_cols], spare, w_sem.at[3])

    small[0].wait()
    first = routes_ref[0:1, :]
    row_group = lax.broadcasted_iota(jnp.int32, (16, tok), 0)
    groups = jnp.full((16, tok), -1, jnp.int32)
    for d in range(Q):
        groups = jnp.where(row_group == d, partner(q, d, Q)[0], groups)
    member = (groups >= 0) & (first >= groups * group_width) & (first < (groups + 1) * group_width)
    earlier = lax.broadcasted_iota(jnp.int32, (tok, tok), 0) < lax.broadcasted_iota(jnp.int32, (tok, tok), 1)
    rank = jnp.dot(
        jnp.where(member, 1.0, 0.0).astype(BF16), jnp.where(earlier, 1.0, 0.0).astype(BF16),
        preferred_element_type=F32,
    ).astype(jnp.int32)
    slots = lax.broadcasted_iota(jnp.int32, (lanes, tok), 0)
    picks = []
    for d in range(Q):
        low = partner(q, d, Q)[0] * group_width
        inside = (first >= low) & (first < low + group_width)
        picks.append(jnp.where((rank[d:d + 1, :] == slots) & inside, 1.0, 0.0))

    tok_copy.wait()
    small[1].wait()
    for copy in [away] + weights:
        copy.start()
    floats = tokens_ref[...].astype(F32)
    inv = lax.rsqrt(jnp.mean(floats * floats, axis=-1, keepdims=True) + EPS)
    normed = (tokens_ref[...].astype(F32) * inv * in_gain_ref[...]).astype(BF16)
    for d in range(Q):
        pick = jnp.where(c == 0, picks[d][:RC], picks[d][RC:R]).astype(BF16)
        block = jnp.dot(pick, normed, preferred_element_type=F32).astype(BF16)
        for h in range(PARTS):
            if d == 0:
                gathered[0, c, h, 0] = block[:, h * W:(h + 1) * W]
            else:
                sendz[d - 1, h] = block[:, h * W:(h + 1) * W]

    pl.semaphore_wait(barrier, N)

    def z_copy(d, h):
        return remote(
            sendz.at[d - 1, h], gathered.at[d, c, h, 0], z_ss, z_rs.at[d - 1, h], at(partner(q, d, Q)[0] * S + s))

    def x_copy(d, e, h):
        return remote(
            gathered.at[d, c, h, 0], gathered.at[d, c, h, e], x_ss, x_rs.at[d, e - 1, h],
            at(q * S + lax.rem(s + e, S)),
        )

    def t_copy(d, e, h):
        block = gathered.at[d, c, h, e]
        return remote(block, block, t_ss, t_rs.at[d], at(me, 1 - c))

    def gate_copy(d, e, near):
        return remote(
            gate_send.at[d, lax.rem(s + e, S)], gate_recv.at[d, e], gate_ss.at[near], gate_rs.at[d],
            at(partner(q, d, Q)[0] * S + lax.rem(s + e, S)),
        )

    def u_copy():
        return remote(spare, w_down.at[1], u_ss, u_rs, at(me, 1 - c))

    def v_copy(d, k):
        return remote(hidden.at[d, k, 0], hidden.at[d, k, 1], v_ss, v_rs.at[d, k], at(me, 1 - c))

    def r_copy(d, e, k):
        return remote(
            r_send.at[d, k, e - 1], r_recv.at[d, k, e - 1], r_ss, r_rs.at[d, k],
            at(q * S + lax.rem(s + S - e, S)),
        )

    def h_copy(d, k):
        return remote(
            home_send.at[d - 1, k], home_recv.at[d, k], h_ss, h_rs.at[d - 1, k], at(partner(q, d, Q)[1] * S + s))

    def forward(d, h):
        loop(1, S, lambda e: x_copy(d, e, h).start())
        t_copy(d, 0, h).start()

    for h in range(PARTS):
        forward(0, h)
    def q_copy(d, k, p):
        home = at(me, 1 - c) if p == 0 else at(partner(q, d, Q)[1] * S + s, 1 - c)
        return remote(sq_send.at[d, k], sq_recv.at[d, k], q_ss, q_rs.at[d, k], home)

    def leave(d):
        for h in range(PARTS):
            z_copy(d, h).start()

    for d in order[:-1]:
        leave(d)

    small[2].wait()
    small[3].wait()
    ids = lax.broadcasted_iota(jnp.int32, (-(-Q * group_width // 16) * 16, tok), 0)
    dense = jnp.zeros(ids.shape, F32)
    for k in range(top):
        dense += jnp.where(routes_ref[k:k + 1, :] == ids, probs_ref[k:k + 1, :], 0.0)
    coarse = dense.astype(BF16)
    fine = (dense - coarse.astype(F32)).astype(BF16)
    for d in range(Q):
        pick = picks[d].astype(BF16)
        lines = sum(
            lax.dot_general(part, pick, (((1,), (1,)), ((), ())), preferred_element_type=F32) for part in (coarse, fine))
        base = partner(q, d, Q)[0]
        mine = jnp.zeros((group_width, lanes), F32)
        for g in range(Q):
            mine = jnp.where(base == g, lines[g * group_width:(g + 1) * group_width], mine)
        for i in range(S):
            gate_send[d, i] = mine[i * L:(i + 1) * L]
    gate_recv[0, 0] = gate_send[0, s]
    for d in range(Q):
        loop(1 if d == 0 else 0, S, lambda e: gate_copy(d, e, int(d == 0)).start())
    leave(order[-1])
    away.wait()
    u_copy().start()

    for d in range(Q):
        for k in range(2):
            unpack[d, k] = picks[d][k * RC:(k + 1) * RC].T.astype(BF16)

    row, lane = (lax.broadcasted_iota(jnp.int32, (RC, lanes), i) for i in (0, 1))

    def up_projection(d, k, n):
        base = n * pair
        tokens = jnp.concatenate(
            [gathered[d, k, h, pl.ds(base, pair)].reshape(rows_at_once, W) for h in range(PARTS)], axis=1)
        at_rows = pl.ds(n * rows_at_once, rows_at_once)
        for j in range(L):
            gate = jnp.dot(tokens, w_gate[j], preferred_element_type=F32)
            up = jnp.dot(tokens, w_up[j], preferred_element_type=F32)
            scale = jnp.concatenate([
                jnp.sum(jnp.where(row + k * RC == lane, gate_recv[d, base + b, pl.ds(j, 1), :], 0.0), axis=1, keepdims=True)
                for b in range(pair)
            ], axis=0)
            act = gate / (1.0 + jnp.exp(-gate)) * up
            hidden[d, k, 0, at_rows, j * F:(j + 1) * F] = (act * scale).astype(BF16)

    def down_projection(d, k, n, ready):
        at_rows = pl.ds(n * rows_at_once, rows_at_once)
        part = jnp.dot(hidden[d, k, 0, at_rows], w_down[0].reshape(L * F, H), preferred_element_type=F32)
        ready()
        return part + jnp.dot(hidden[d, k, 1, at_rows], w_down[1].reshape(L * F, H), preferred_element_type=F32)

    def arrived(block, sem):
        remote(block, block, sem, sem, at(me, 1 - c)).wait_recv()

    def sent(block, sem):
        remote(block, block, sem, sem, at(me, 1 - c)).wait_send()

    ups_left = [(p, k) for p in range(Q) for k in range(2)]
    down_ready, gates_ready, mixed_ready, unsent = [], [], [], []

    def send_squares():
        units = list(unsent)
        unsent.clear()
        for p, k in units:
            d = place[p]
            rows = (home_recv[0, k] if p == 0 else home_send[d - 1, k]).astype(F32)
            squares = rows * rows
            squares = sum(squares[:, i:i + 128] for i in range(128, H, 128)) + squares[:, :128]
            line = lax.dot_general(
                jnp.ones((8, 128), F32), squares, (((1,), (1,)), ((), ())),
                precision=lax.Precision.HIGHEST, preferred_element_type=F32)
            sq_send[d, k, :, :RC] = line[:1]
        for p, k in units:
            q_copy(place[p], k, p).start()

    def step_a(p, k):
        d = place[p]

        @pl.when(c == k)
        def _():
            for h in range(PARTS):
                z_copy(d, h).wait_recv()
                forward(d, h)

    def step_b(p, k):
        d = place[p]

        def one(e):
            for h in range(PARTS):
                x_copy(d, e, h).wait_recv()
                t_copy(d, e, h).start()
        pl.when(c == k)(lambda: loop(1, S, one))

    def step_g(p, k):
        d = place[p]
        ups_left.remove((p, k))
        if not gates_ready:
            for copy in weights:
                copy.wait()
        if p not in gates_ready:
            arrived(gate_recv.at[d, pl.ds(1, S - 1)] if p == 0 else gate_recv.at[d], gate_rs.at[d])
            gates_ready.append(p)

        pl.when(c != k)(lambda: arrived(gathered.at[d, 1 - c], t_rs.at[d]))
        if S == pair:
            up_projection(d, k, 0)
        else:
            lax.fori_loop(0, S // pair, lambda n, carry: (up_projection(d, k, n), carry)[1], 0)
        v_copy(d, k).start()
        send_squares()

    def step_d(p, k):
        d = place[p]
        if not down_ready:
            u_copy().wait_recv()
            down_ready.append(True)
        out = down_projection(d, k, 0, v_copy(d, k).wait_recv)
        for e in range(1, pair):
            r_send[d, k, e - 1] = out[e * RC:(e + 1) * RC].astype(BF16)
        own_sum[d, k] = out[:RC]
        if S > pair:
            def some(n, carry):
                out = down_projection(d, k, n, lambda: None)
                r_send[d, k, pl.ds(n * pair - 1, pair)] = out.astype(BF16).reshape(pair, RC, H)
                return carry
            lax.fori_loop(1, S // pair, some, 0)
        loop(1, S, lambda e: r_copy(d, e, k).start())

    def step_f(p, k):
        d = place[p]

        arrived(r_recv.at[d, k], r_rs.at[d, k])
        total = own_sum[d, k]
        if S <= 8:
            for e in range(1, S):
                total = total + r_recv[d, k, e - 1].astype(F32)
        else:
            total = lax.fori_loop(1, S, lambda e, total: total + r_recv[d, k, e - 1].astype(F32), total)
        if p == 0:
            home_recv[0, k] = total.astype(BF16)
        else:
            home_send[d - 1, k] = total.astype(BF16)
            h_copy(d, k).start()
        unsent.append((p, k))
        if not ups_left:
            send_squares()

    def step_m(p, k):
        d = place[p]
        if p > 0:
            h_copy(d, k).wait_recv()
        term = jnp.dot(unpack[d, k], home_recv[d, k], preferred_element_type=F32)
        mixed[...] = mixed[...] + term if mixed_ready else term
        mixed_ready.append(True)

    actions = {"A": step_a, "B": step_b, "G": step_g, "D": step_d, "F": step_f, "M": step_m}

    steps = STEPS
    if Q != 4:
        units = [f"{p}{k}" for p in range(Q) for k in (1, 0)]
        steps = ["A" + u for u in units[2:]] + [x + u for x in "BGDFM" for u in units]
    for step in steps:
        actions[step[0]](*(int(i) for i in step[1:]))

    total = mixed[...]
    squares = jnp.sum(total * total, axis=1, keepdims=True)
    u_copy().wait_send()
    sent(gate_send.at[pl.ds(1, Q - 1)], gate_ss.at[0])
    sent(gate_send.at[0, pl.ds(1, S - 1)], gate_ss.at[1])
    sent(sendz, z_ss)
    sent(gathered.at[:, c, :, pl.ds(1, S - 1)], x_ss)
    sent(gathered.at[:, c], t_ss)
    sent(hidden.at[:, :, 0], v_ss)
    sent(r_send, r_ss)
    sent(home_send, h_ss)
    sent(sq_send, q_ss)
    theirs = jnp.zeros((tok, RC), F32)
    for p in range(Q):
        for k in range(2):
            q_copy(place[p], k, p).wait_recv()
            theirs += unpack[place[p], k].astype(F32) * sq_recv[place[p], k, :, :RC]
    squares = squares + jnp.sum(theirs, axis=1, keepdims=True)
    out_ref[...] = (total * lax.rsqrt(squares / width + EPS) * out_gain_ref[...]).astype(BF16)


def body(tokens, in_gain, routing, gate_prob, w_gate, w_up, w_down, out_gain):
    N = lax.axis_size("ep")
    L, D, F = w_gate.shape
    tok, top = routing.shape
    H = out_gain.shape[0]
    group_width = L * N // GROUPS
    cap = max(2, tok * top // (2 * group_width))
    R = min(tok, group_width * cap // top)
    R = -(-R // 16) * 16
    Q, S, K = GROUPS, N // GROUPS, 2
    RC = R // K
    lanes = -(-R // 128) * 128
    vmem = pl.BlockSpec(memory_space=pltpu.VMEM)
    hbm = pl.BlockSpec(memory_space=pl.ANY)
    dma = pltpu.SemaphoreType.DMA
    return pl.pallas_call(
        functools.partial(kernel, Q, S, R),
        out_shape=pltpu.VMEM((tok, H), BF16),
        in_specs=[hbm] * 8,
        out_specs=vmem,
        scratch_shapes=[
            pltpu.VMEM((top, tok), jnp.int32),
            pltpu.VMEM((top, tok), F32),
            pltpu.VMEM((1, D), F32),
            pltpu.VMEM((1, H), F32),
            pltpu.VMEM((tok, D), BF16),
            pltpu.VMEM((Q - 1, PARTS, RC, D // PARTS), BF16),
            pltpu.VMEM((Q, K, PARTS, S, RC, D // PARTS), BF16),
            pltpu.VMEM((Q, K, tok, RC), BF16),
            pltpu.VMEM((Q, S, L, lanes), F32),
            pltpu.VMEM((Q, S, L, lanes), F32),
            pltpu.VMEM((L, D, F), BF16),
            pltpu.VMEM((L, D, F), BF16),
            pltpu.VMEM((2, L, F, H), BF16),
            pltpu.VMEM((L, F, H), BF16),
            pltpu.VMEM((Q, K, 2, S * RC, L * F), BF16),
            pltpu.VMEM((Q, K, S - 1, RC, H), BF16),
            pltpu.VMEM((Q, K, RC, H), F32),
            pltpu.VMEM((Q, K, S - 1, RC, H), BF16),
            pltpu.VMEM((Q - 1, K, RC, H), BF16),
            pltpu.VMEM((Q, K, RC, H), BF16),
            pltpu.VMEM((tok, H), F32),
            pltpu.VMEM((Q, K, 1, lanes), F32),
            pltpu.VMEM((Q, K, 1, lanes), F32),
            dma((5,)), dma((4,)), dma((2,)), dma((Q,)), dma, dma((Q - 1, PARTS)), dma, dma((Q, S - 1, PARTS)),
            dma, dma((Q,)), dma, dma, dma, dma((Q, K)), dma, dma((Q, K)), dma, dma((Q - 1, K)), dma, dma((Q, K)),
        ],
        compiler_params=pltpu.CompilerParams(
            collective_id=0, has_side_effects=True, vmem_limit_bytes=64 * 1000 * 1000
        ),
    )(routing.T, gate_prob.T, in_gain.reshape(1, D), out_gain.reshape(1, H), tokens, w_gate, w_up, w_down)


def solution(mesh):
    placed = (
        P(("grp", "ep"), None),
        P(),
        P(("grp", "ep"), None),
        P(("grp", "ep"), None),
        P("ep", None, "tp"),
        P("ep", None, "tp"),
        P("ep", "tp", None),
        P("tp"),
    )
    return jax.shard_map(
        body, mesh=mesh, in_specs=placed, out_specs=P(("grp", "ep"), "tp"), check_vma=False
    )
```
